32 devices in a mesh: ep: 8 (over z, y), tp: 4 (over x, core).
Axes of the slice: x: 2, y: 2, z: 4, core: 2. Of those that a mesh axis runs over, the one named last changes fastest.
Arguments:
- tokens: bfloat16 [1344, 2048], P('ep'), may hold values from -6 to 6
- cotangent: bfloat16 [1344, 2048], P('ep'), may hold values from -6 to 6
- group_ids: int32 [1344, 1], P('ep'), may hold values from 0 to 7; in each aligned block of 168 rows (0 to 167, 168 to 335, ...) at most 32 rows name the same one
- within_ids: int32 [1344, 2], P('ep'), may hold values from 0 to 1, all different within a row
- gate_weights: bfloat16 [1344, 2], P('ep'), may hold values from 0.099609375 to 1
- w_gate: bfloat16 [16, 2048, 1024], P('ep', None, 'tp'), may hold values from -0.125 to 0.125
- w_up: bfloat16 [16, 2048, 1024], P('ep', None, 'tp'), may hold values from -0.125 to 0.125
- w_down: bfloat16 [16, 1024, 2048], P('ep', 'tp'), may hold values from -0.1875 to 0.1875
Outputs:
- tokens_grad: bfloat16 [1344, 2048], P('ep', 'tp')
- gate_grad: float32 [1344, 2], P('ep')
- w_gate_grad: bfloat16 [16, 2048, 1024], P('ep', None, 'tp')
- w_up_grad: bfloat16 [16, 2048, 1024], P('ep', None, 'tp')
- w_down_grad: bfloat16 [16, 1024, 2048], P('ep', 'tp')
The draws below stay inside these ranges and needn't reach their ends.
Inputs may be any that keep to these rules, and one draw needn't show every extreme that they name: `group_ids`: in the rows of one device no group is chosen by more than 32 rows. `within_ids`: the two entries of a row differ.
All inputs are finite; a program needn't handle non-finite values.
Results may differ from the reference program's by a relative error of at most 0.017.
Values may be sent and summed in bfloat16 or wider, within the bound.
A program may use at most 64 MiB of HBM per device.

```python
import math
import jax
import jax.numpy as jnp
import numpy as np
from jax import lax

D = 2048
FF = 1024
GROUP_EXPERTS = 2
TOP_K = 2
TOK_DEV = 168
GROUPS = 8
EXPERTS = 16
CAP = 32
TOKENS = 1344
N_EP = 8
N_TP = 4


def steps_of(stream_key, shape, shards, least, largest):
    loudness, own = 1.0, jax.random.fold_in(stream_key, 6)
    for position, shards_of in shards:
        steps = jnp.exp(jax.random.uniform(jax.random.fold_in(own, position), (shards_of,), jnp.float32, least / len(shards), largest / len(shards)))
        loudness = loudness * jnp.repeat(steps, shape[position] // shards_of).reshape([-1 if axis == position else 1 for axis in range(len(shape))])
    return loudness


def different_ones(stream_key, rows, number_of, top, lift):
    ranking = jax.random.permutation(jax.random.fold_in(stream_key, 1), number_of)
    pull = ranking
    for power in range(3):
        pull = pull * pull // number_of
    pull = pull * lift // number_of
    tickets = jax.random.randint(jax.random.fold_in(stream_key, 2), (rows, number_of), 0, 4096) + pull
    sure = jax.random.permutation(jax.random.fold_in(stream_key, 3), rows)[jnp.arange(number_of) % rows]
    tickets = jnp.where(jnp.arange(rows)[:, None] == sure[None, :], 1 << 14, tickets)
    score = tickets * number_of + jnp.arange(number_of)
    return lax.top_k(score.astype(jnp.int32), top)[1].astype(jnp.int32)


def routed_block(rng, own, number, rows, count, top, bound, lean):
    ranking = jax.random.permutation(rng, count)
    packed, usual = portions_of(count, rows * top, bound, lean, True), portions_of(count, rows * top, bound, lean, False)
    places = jnp.arange(count)

    def named(sizes, turn):
        used = int((sizes > 0).sum())
        fixed = max(1, used // 4)
        moved = fixed + (places - fixed + turn * (used - fixed)) % max(1, count - fixed)
        return jnp.zeros((count,), jnp.int32).at[ranking[jnp.where(places < fixed, places, moved)]].set(jnp.asarray(sizes, jnp.int32))

    sizes = jnp.where(number % 4 == 0, named(packed, number // 4), named(usual, number - number // 4 - 1))
    mixed = jax.random.permutation(jax.random.fold_in(own, 3), count)
    source_of, receiver = mixed[0:count // 2 * 2:2], mixed[1:count // 2 * 2:2]
    margin = jnp.minimum(sizes[source_of] - 1, bound - sizes[receiver]) // 2
    margin = jnp.where((source_of == ranking[0]) | (receiver == ranking[0]) | (sizes[receiver] == 0), 0, jnp.maximum(margin, 0))
    moved = jax.random.randint(jax.random.fold_in(own, 4), (count // 2,), 0, 1 << 20) % (margin + 1)
    sizes = sizes.at[source_of].add(-moved).at[receiver].add(moved)
    items = jnp.searchsorted(jnp.cumsum(sizes), jnp.arange(rows * top), side="right").astype(jnp.int32)
    grid = items.reshape(top, rows).T
    grid = grid[jax.random.permutation(jax.random.fold_in(own, 1), rows)]
    turn = jax.random.randint(jax.random.fold_in(own, 2), (rows, 1), 0, top)
    return jnp.take_along_axis(grid, (jnp.arange(top)[None, :] + turn) % top, axis=1)


def portions_of(number_of, total, bound, lean, full):
    loads = [(1 << 20) // math.isqrt(rank ** lean) + 1 for rank in range(1, number_of + 1)]
    largest = bound if full else min(bound, max(-(-total // number_of), total * loads[0] // sum(loads)))
    least = 1 if total - largest >= number_of - 1 else 0
    counts, spare = [largest] + [least] * (number_of - 1), total - largest - least * (number_of - 1)
    while spare > 0:
        free = [i for i in range(1, number_of) if counts[i] < largest] or [i for i in range(1, number_of) if counts[i] < bound]
        mass, remaining = sum([loads[i] for i in free]), spare
        for i in free:
            more = min(bound - counts[i], max(1, remaining * loads[i] // mass), spare)
            counts[i] = counts[i] + more
            spare = spare - more
    return np.array(counts)


def noise(stream_key, dims, spread, bound, pieces=(), kind=jnp.bfloat16):
    gain = steps_of(stream_key, dims, pieces, -0.22, 0.18) if pieces else 1.0
    array = jax.random.normal(stream_key, dims, jnp.float32) * spread * gain
    return jnp.minimum(jnp.maximum(array, -bound), bound).astype(kind)


def setup_inputs(seed: int = 0) -> dict:
    splits = jax.random.split(jax.random.key(seed), 9)
    tokens = noise(splits[0], (TOKENS, D), 1.0, 6.0, ((0, 8),))
    cotangent = noise(splits[1], (TOKENS, D), 1.0, 6.0, ((0, 8),))
    group_ids_keys = jax.random.split(jax.random.fold_in(splits[2], 1), TOKENS // TOK_DEV)
    group_ids_turns = jax.random.permutation(jax.random.fold_in(splits[2], 3), TOKENS // TOK_DEV)
    group_ids = jax.vmap(lambda own, number: routed_block(jax.random.fold_in(splits[2], 2), own, number, TOK_DEV, GROUPS, 1, CAP, 2))(group_ids_keys, group_ids_turns).reshape((TOKENS, 1))
    within_ids = different_ones(splits[3], TOKENS, GROUP_EXPERTS, TOP_K, 8192)
    gate_weights = jnp.clip(jnp.exp(math.log(1.0) - 2.306499 * jax.random.uniform(splits[4], (TOKENS, TOP_K), jnp.float32) ** steps_of(splits[4], (TOKENS, TOP_K), ((0, 8),), -0.2, 0.2)), 0.099609375, 1.0).astype(jnp.bfloat16)
    w_gate = noise(splits[5], (EXPERTS, D, FF), D ** -0.5, 0.125, ((0, 8), (2, 4)))
    w_up = noise(splits[6], (EXPERTS, D, FF), D ** -0.5, 0.125, ((0, 8), (2, 4)))
    w_down = noise(splits[7], (EXPERTS, FF, D), FF ** -0.5, 0.1875, ((0, 8), (1, 4)))
    return {"tokens": tokens, "cotangent": cotangent, "group_ids": group_ids, "within_ids": within_ids, "gate_weights": gate_weights, "w_gate": w_gate, "w_up": w_up, "w_down": w_down}


def reference(tokens, cotangent, group_ids, within_ids, gate_weights, w_gate, w_up, w_down):
    rows_max = N_EP * CAP
    ff_local = FF // N_TP
    group_of = group_ids[:, 0]
    sorted_rows = jnp.argsort(group_of, stable=True).astype(jnp.int32)
    in_group = (group_of[:, None] == jnp.arange(GROUPS, dtype=jnp.int32)[None, :]).astype(jnp.int32)
    group_counts = jnp.sum(in_group, axis=0)
    offsets = jnp.cumsum(group_counts) - group_counts
    local_ids = jnp.arange(GROUP_EXPERTS, dtype=jnp.int32)
    chosen = (within_ids[:, :, None] == local_ids[None, None, :]).astype(jnp.float32)
    combine = jnp.sum(chosen * gate_weights.astype(jnp.float32)[:, :, None], axis=1).astype(jnp.bfloat16)

    def one_group(group_index):
        positions = jnp.arange(rows_max, dtype=jnp.int32)
        is_valid = positions < group_counts[group_index]
        row_ids = sorted_rows[jnp.clip(offsets[group_index] + positions, 0, TOKENS - 1)]
        keep = is_valid[:, None]
        slot_x = jnp.where(keep, tokens[row_ids], jnp.zeros((), jnp.bfloat16))
        slot_dy = jnp.where(keep, cotangent[row_ids], jnp.zeros((), jnp.bfloat16))
        slot_comb = jnp.where(keep, combine[row_ids], jnp.zeros((), jnp.bfloat16))
        first = (group_index * GROUP_EXPERTS).astype(jnp.int32)
        local_gate = lax.dynamic_slice_in_dim(w_gate, first, GROUP_EXPERTS, 0)
        local_up = lax.dynamic_slice_in_dim(w_up, first, GROUP_EXPERTS, 0)
        local_down = lax.dynamic_slice_in_dim(w_down, first, GROUP_EXPERTS, 0)
        dy_float = slot_dy.astype(jnp.float32)
        blocks = jnp.zeros((N_TP, rows_max, D), jnp.float32)
        gate_parts = []
        grads_gate = []
        grads_up = []
        grads_down = []
        for expert in range(GROUP_EXPERTS):
            pre_gate = jnp.dot(slot_x, local_gate[expert], preferred_element_type=jnp.float32)
            pre_up = jnp.dot(slot_x, local_up[expert], preferred_element_type=jnp.float32)
            sig_gate = jax.nn.sigmoid(pre_gate)
            act_b = (pre_gate * sig_gate * pre_up).astype(jnp.bfloat16)
            down = jnp.dot(act_b, local_down[expert], preferred_element_type=jnp.float32)
            gate_parts.append(jnp.sum(dy_float * down, axis=1))
            scaled = (slot_comb[:, expert:expert + 1].astype(jnp.float32) * dy_float).astype(jnp.bfloat16)
            grads_down.append(jnp.dot(act_b.T, scaled, preferred_element_type=jnp.float32).astype(jnp.bfloat16))
            act_grad = jnp.dot(scaled, local_down[expert].T, preferred_element_type=jnp.float32)
            gate_b = (act_grad * pre_up * sig_gate * (1.0 + pre_gate * (1.0 - sig_gate))).astype(jnp.bfloat16)
            up_b = (act_grad * pre_gate * sig_gate).astype(jnp.bfloat16)
            grads_gate.append(jnp.dot(slot_x.T, gate_b, preferred_element_type=jnp.float32).astype(jnp.bfloat16))
            grads_up.append(jnp.dot(slot_x.T, up_b, preferred_element_type=jnp.float32).astype(jnp.bfloat16))
            gate_split = gate_b.astype(jnp.float32).reshape(rows_max, N_TP, ff_local)
            up_split = up_b.astype(jnp.float32).reshape(rows_max, N_TP, ff_local)
            wg_split = local_gate[expert].astype(jnp.float32).reshape(D, N_TP, ff_local)
            wu_split = local_up[expert].astype(jnp.float32).reshape(D, N_TP, ff_local)
            blocks = blocks + jnp.einsum('rnf,dnf->nrd', gate_split, wg_split)
            blocks = blocks + jnp.einsum('rnf,dnf->nrd', up_split, wu_split)
        rounded = lax.optimization_barrier(blocks.astype(jnp.bfloat16)).astype(jnp.float32)
        dx_rows = jnp.sum(rounded, axis=0).astype(jnp.bfloat16)
        return (dx_rows, jnp.stack(gate_parts, axis=1), row_ids, is_valid,
                jnp.stack(grads_gate), jnp.stack(grads_up), jnp.stack(grads_down))

    dx_all, gate_all, rows_all, valid_all, gg_all, gu_all, gd_all = lax.map(
        one_group, jnp.arange(GROUPS, dtype=jnp.int32))
    flat_rows = rows_all.reshape(-1)
    flat_valid = valid_all.reshape(-1)[:, None]
    dx_flat = jnp.where(flat_valid, dx_all.reshape(-1, D).astype(jnp.float32), 0.0)
    tokens_grad = jnp.zeros((TOKENS, D), jnp.float32).at[flat_rows].add(dx_flat).astype(jnp.bfloat16)
    gate_flat = jnp.where(flat_valid, gate_all.reshape(-1, GROUP_EXPERTS), 0.0)
    dense_gate = jnp.zeros((TOKENS, GROUP_EXPERTS), jnp.float32).at[flat_rows].add(gate_flat)
    gate_grad = jnp.sum(chosen * dense_gate[:, None, :], axis=2)
    w_gate_grad = gg_all.reshape(EXPERTS, D, FF)
    w_up_grad = gu_all.reshape(EXPERTS, D, FF)
    w_down_grad = gd_all.reshape(EXPERTS, FF, D)
    return tokens_grad, gate_grad, w_gate_grad, w_up_grad, w_down_grad
```

```python
import functools

import jax
import jax.numpy as jnp
from jax import lax
from jax.experimental import pallas as pl
from jax.experimental.pallas import tpu as pltpu
from jax.sharding import PartitionSpec as P

MESH = pl.DeviceIdType.MESH
LANES = 128
NT = (((1,), (1,)), ((), ()))
TN = (((0,), (0,)), ((), ()))
NN = (((1,), (0,)), ((), ()))


def dot(a, b, dims=NN):
    return lax.dot_general(a, b, dims, preferred_element_type=jnp.float32)


def each(count, body):
    if count <= 8:
        for i in range(count):
            body(i)
    else:
        lax.fori_loop(0, count, lambda i, c: (body(i), c)[1], 0)


def aligned(value, step):
    return value if isinstance(value, int) else pl.multiple_of(value, step)


def kernel(
    ep, tp, cap,
    tok_ref, cot_ref, gid_ref, wid_ref, gw_ref, wg_ref, wu_ref, wd_ref,
    place_ref, back, gate_back, vwg, vwu, vwd,
    src, placed, rows_in, wg, wu, wd, acc, gate_b, up_b, act_c,
    to_partner, from_partner, dx_acc, to_x, from_x, to_ep,
    gate_in, gate_sum,
    load_sem, own_sem, send1, recv_rows, send_x, send_p, send_p2,
    dxp_send, dxp_recv, dxx_send, dxx_recv, dxe_send, dxe_recv,
    gt_send, gt_recv, ge_send, ge_recv,
):
    e_me = lax.axis_index("ep")
    t_me = lax.axis_index("tp")
    core = lax.rem(t_me, 2)
    x_me = lax.div(t_me, 2)
    partner = t_me + 1 - 2 * core
    nx = tp // 2
    gate_lanes = gate_back.shape[2]
    tok_rows, width = tok_ref.shape
    cs = width // tp
    slots = ep * cap
    experts = wg.shape[0]
    bf16 = jnp.bfloat16

    barrier = pltpu.get_barrier_semaphore()
    each(ep - 1, lambda i: pl.semaphore_signal(
        barrier, inc=1, device_id=(lax.rem(e_me + 1 + i, ep), t_me), device_id_type=MESH))
    each(tp - 1, lambda i: pl.semaphore_signal(
        barrier, inc=1, device_id=(e_me, lax.rem(t_me + 1 + i, tp)), device_id_type=MESH))

    my_cols = pl.ds(pl.multiple_of(t_me * cs, LANES), cs)
    loads = [
        pltpu.make_async_copy(tok_ref.at[:, my_cols], src.at[:, pl.ds(0, cs)], load_sem.at[0]),
        pltpu.make_async_copy(cot_ref.at[:, my_cols], src.at[:, pl.ds(cs, cs)], load_sem.at[1]),
        pltpu.make_async_copy(wg_ref, wg, load_sem.at[2]),
        pltpu.make_async_copy(wu_ref, wu, load_sem.at[3]),
        pltpu.make_async_copy(wd_ref, wd, load_sem.at[4]),
    ]
    for load in loads[:2]:
        load.start()

    group = gid_ref[...]
    groups = -(-ep // 16) * 16
    in_group = (
        lax.broadcasted_iota(jnp.int32, (groups, tok_rows), 0) == group
    ).astype(jnp.float32)
    earlier = (
        lax.broadcasted_iota(jnp.int32, (tok_rows, tok_rows), 0)
        < lax.broadcasted_iota(jnp.int32, (tok_rows, tok_rows), 1)
    ).astype(jnp.float32).astype(bf16)
    before = dot(in_group.astype(bf16), earlier)
    rank = jnp.sum(before * in_group, axis=0, keepdims=True).astype(jnp.int32)
    slot_row = lax.broadcasted_iota(jnp.int32, (slots, tok_rows), 0)
    place = (slot_row == group * cap + rank).astype(jnp.float32).astype(bf16)
    place_ref[0] = place
    place_ref[1] = (slot_row == e_me * cap % gate_lanes + rank).astype(jnp.float32).astype(bf16)
    lane_row = lax.broadcasted_iota(jnp.int32, (LANES, tok_rows), 0)
    weights = gw_ref[...].astype(jnp.float32)
    comb = jnp.zeros((LANES, tok_rows), jnp.float32)
    for k in range(weights.shape[0]):
        comb = comb + jnp.where(lane_row == wid_ref[k : k + 1, :], weights[k : k + 1, :], 0.0)
    placed[:, pl.ds(2 * cs, LANES)] = dot(place, comb.astype(bf16), NT).astype(bf16)
    loads[0].wait()
    placed[:, pl.ds(0, cs)] = dot(place, src[:, pl.ds(0, cs)]).astype(bf16)
    loads[1].wait()
    for load in loads[2:]:
        load.start()
    placed[:, pl.ds(cs, cs)] = dot(place, src[:, pl.ds(cs, cs)]).astype(bf16)

    pl.semaphore_wait(barrier, ep + tp - 2)

    def xor(d):
        value, bit = 0, 1
        while bit < ep:
            value = value + (e_me // bit + d // bit) % 2 * bit
            bit *= 2
        return value

    def target(d):
        return xor(d) if ep & (ep - 1) == 0 else lax.rem(e_me + d, ep)

    def source(d):
        return xor(d) if ep & (ep - 1) == 0 else lax.rem(e_me - d + ep, ep)

    def block(e):
        return pl.ds(aligned(e * cap, 16), cap)

    distances = list(range(ep))
    def stage1(d):
        g = target(d)
        return pltpu.make_async_remote_copy(
            src_ref=placed.at[block(g)], dst_ref=rows_in.at[t_me, block(e_me)],
            send_sem=send1.at[d], recv_sem=recv_rows.at[t_me, e_me],
            device_id=(g, t_me), device_id_type=MESH)

    own = pltpu.make_async_copy(
        placed.at[block(e_me)], rows_in.at[t_me, block(e_me)], own_sem.at[0])
    own.start()
    if ep <= 8:
        for d in distances[1:]:
            stage1(d).start()
    else:
        each(ep - 1, lambda i: stage1(i + 1).start())

    def arrived(q, e, cols):
        part = rows_in.at[q, block(e), pl.ds(0, cols)]
        pltpu.make_async_remote_copy(
            src_ref=part, dst_ref=part, send_sem=send1.at[0], recv_sem=recv_rows.at[q, e],
            device_id=(e_me, partner), device_id_type=MESH).wait_recv()

    def forward(q, e, sem, target):
        part = rows_in.at[q, block(e), pl.ds(0, 2 * cs)]
        return pltpu.make_async_remote_copy(
            src_ref=part, dst_ref=part, send_sem=sem, recv_sem=recv_rows.at[q, e],
            device_id=(e_me, target), device_id_type=MESH)

    def x_peer(k):
        return lax.rem(x_me + k, nx) * 2 + core

    def to_peers(d):
        e = source(d)
        copies = [forward(t_me, e, send_x.at[k - 1, d], x_peer(k)) for k in range(1, nx)]
        return copies + [forward(t_me, e, send_p.at[d], partner)]

    def stage2(d):
        for copy in to_peers(d):
            copy.start()

    def relays(d):
        e = source(d)
        return [(x_peer(k), e, forward(x_peer(k), e, send_p2.at[k - 1, d], partner))
                for k in range(1, nx)]

    def stage3(d):
        for q, e, copy in relays(d):
            arrived(q, e, 2 * cs)
            copy.start()

    own.wait()
    stage2(0)
    if ep <= 8:
        for i, d in enumerate(distances[1:]):
            arrived(t_me, source(d), 2 * cs + LANES)
            stage2(d)
    else:
        def later(i):
            arrived(t_me, source(i + 1), 2 * cs + LANES)
            stage2(i + 1)
        each(ep - 1, later)

    for load in loads[2:]:
        load.wait()

    def share(q):
        return pl.ds(aligned(q * cs, LANES), cs)

    def hidden(q, first):
        xq = rows_in[q, :, pl.ds(0, cs)]
        yq = rows_in[q, :, pl.ds(cs, cs)]
        for e in range(experts):
            for n, value in enumerate((
                dot(xq, wg[e, share(q), :]),
                dot(xq, wu[e, share(q), :]),
                dot(yq, wd[e, :, share(q)], NT),
            )):
                acc[e, n] = value if first else acc[e, n] + value

    def all_arrived(q):
        each(ep, lambda e: arrived(q, e, 2 * cs))

    hidden(t_me, True)
    if ep <= 8:
        for d in distances:
            stage3(d)
    else:
        each(ep, stage3)
    all_arrived(partner)
    hidden(partner, False)

    def x_quarters(k):
        hidden(x_peer(k), False)
        other = lax.rem(x_me + k, nx) * 2 + 1 - core
        all_arrived(other)
        hidden(other, False)
    each(nx - 1, lambda i: x_quarters(i + 1))

    row8 = lax.broadcasted_iota(jnp.int32, (8, slots), 0)
    gates = jnp.zeros((8, slots), jnp.float32)
    for e in range(experts):
        pre_gate, pre_up, dy_down = acc[e, 0], acc[e, 1], acc[e, 2]
        c = rows_in[t_me, :, pl.ds(2 * cs, LANES)][:, e : e + 1].astype(jnp.float32)
        sig = jax.nn.sigmoid(pre_gate)
        silu = pre_gate * sig
        act = silu * pre_up
        prod = act.astype(bf16).astype(jnp.float32) * dy_down
        act_grad = c * dy_down
        act_c[e] = (c * act).astype(bf16)
        gate_b[e] = (act_grad * pre_up * sig * (1.0 + pre_gate * (1.0 - sig))).astype(bf16)
        up_b[e] = (act_grad * silu).astype(bf16)
        high = prod.astype(bf16)
        low = (prod - high.astype(jnp.float32)).astype(bf16)
        ones = jnp.ones((8, prod.shape[1]), bf16)
        gates = gates + jnp.where(row8 == e, dot(ones, high, NT) + dot(ones, low, NT), 0.0)
    gate_in[t_me] = gates

    def gate_tp(i):
        return pltpu.make_async_remote_copy(
            src_ref=gate_in.at[t_me], dst_ref=gate_in.at[t_me],
            send_sem=gt_send.at[i], recv_sem=gt_recv.at[t_me],
            device_id=(e_me, lax.rem(t_me + 1 + i, tp)), device_id_type=MESH)

    def dx_of(q):
        total = None
        for e in range(experts):
            part = dot(gate_b[e], wg[e, share(q), :], NT) + dot(up_b[e], wu[e, share(q), :], NT)
            total = part if total is None else total + part
        return total

    def dx_partner(k):
        return pltpu.make_async_remote_copy(
            src_ref=to_partner.at[k], dst_ref=from_partner.at[k],
            send_sem=dxp_send.at[k], recv_sem=dxp_recv.at[k],
            device_id=(e_me, partner), device_id_type=MESH)

    def give_partner(i):
        k = nx - 1 - i
        to_partner[k] = dx_of(lax.rem(x_me + k, nx) * 2 + 1 - core).astype(bf16)
        dx_partner(k).start()

    def dx_x(k, d):
        e = target(d)
        return pltpu.make_async_remote_copy(
            src_ref=to_x.at[k - 1, block(e)], dst_ref=from_x.at[k - 1, block(e)],
            send_sem=dxx_send.at[k - 1, d], recv_sem=dxx_recv.at[k - 1, d],
            device_id=(e_me, x_peer(k)), device_id_type=MESH)

    far = distances[::-1]

    def walk(body):
        if ep <= 8:
            for i, d in enumerate(far):
                body(i, d)
        else:
            each(ep, lambda i: body(i, ep - 1 - i))

    def give_x(k):
        mine = dx_of(x_peer(k))
        dx_partner(k).wait_recv()
        to_x[k - 1] = (mine + from_partner[k].astype(jnp.float32)).astype(bf16)
        walk(lambda i, d: dx_x(k, d).start())
    each(tp - 1, lambda i: gate_tp(i).start())

    def cross(i):
        give_partner(i)
        give_x(nx - 1 - i)
    each(nx - 1, cross)
    give_partner(nx - 1)
    mine = dx_of(t_me)
    dx_partner(0).wait_recv()
    dx_acc[...] = mine + from_partner[0].astype(jnp.float32)

    def gate_tile(e):
        return pl.ds(pl.multiple_of(e * cap // gate_lanes * gate_lanes, LANES), gate_lanes)

    def gate_ep(d):
        return pltpu.make_async_remote_copy(
            src_ref=gate_sum.at[:, gate_tile(target(d))], dst_ref=gate_back.at[e_me],
            send_sem=ge_send.at[d], recv_sem=ge_recv.at[e_me],
            device_id=(target(d), t_me), device_id_type=MESH)

    def gate_wait(i):
        q = lax.rem(t_me + 1 + i, tp)
        pltpu.make_async_remote_copy(
            src_ref=gate_in.at[q], dst_ref=gate_in.at[q],
            send_sem=gt_send.at[i], recv_sem=gt_recv.at[q],
            device_id=(e_me, q), device_id_type=MESH).wait_recv()

    def gates_on():
        each(tp - 1, gate_wait)
        total = gate_in[0]
        for q in range(1, tp):
            total = total + gate_in[q]
        gate_sum[...] = total
        gate_back[e_me] = gate_sum[:, gate_tile(e_me)]
        each(ep - 1, lambda i: gate_ep(i + 1).start())

    def weight_grads(q):
        x_t = rows_in[q, :, pl.ds(0, cs)].T
        yq = rows_in[q, :, pl.ds(cs, cs)]
        for e in range(experts):
            vwg[e, share(q), :] = dot(x_t, gate_b[e]).astype(bf16)
            vwu[e, share(q), :] = dot(x_t, up_b[e]).astype(bf16)
            vwd[e, :, share(q)] = dot(act_c[e], yq, TN).astype(bf16)

    def dx_ep(d):
        g = target(d)
        return pltpu.make_async_remote_copy(
            src_ref=to_ep.at[block(g)], dst_ref=back.at[block(e_me)],
            send_sem=dxe_send.at[d], recv_sem=dxe_recv.at[e_me],
            device_id=(g, t_me), device_id_type=MESH)

    def finish_chunk(d):
        rows = block(target(d))
        value = dx_acc[rows, :]
        for k in range(1, nx):
            dx_x(k, d).wait_recv()
            value = value + from_x[k - 1, rows, :].astype(jnp.float32)
        return value.astype(bf16)

    def chunk(i, d):
        to_ep[block(target(d)), :] = finish_chunk(d)
        dx_ep(d).start()

    if ep <= 8:
        done = 0
        for i, d in enumerate(far[:-1]):
            chunk(i, d)
            if i % 2 == 0 and done < tp:
                weight_grads(done)
                done += 1
            if i == min(2, ep - 2):
                gates_on()
        for q in range(done, tp):
            weight_grads(q)
    else:
        each(ep - 1, lambda i: chunk(i, ep - 1 - i))
        each(tp, weight_grads)
        gates_on()
    back[block(e_me), :] = finish_chunk(0)

    def gate_arrived(i):
        g = lax.rem(e_me + 1 + i, ep)
        pltpu.make_async_remote_copy(
            src_ref=gate_sum.at[:, gate_tile(g)], dst_ref=gate_back.at[g],
            send_sem=ge_send.at[0], recv_sem=ge_recv.at[g],
            device_id=(g, t_me), device_id_type=MESH).wait_recv()
    each(ep - 1, gate_arrived)
    def back_arrived(i):
        g = lax.rem(e_me + 1 + i, ep)
        pltpu.make_async_remote_copy(
            src_ref=to_ep.at[block(g)], dst_ref=back.at[block(g)],
            send_sem=dxe_send.at[0], recv_sem=dxe_recv.at[g],
            device_id=(g, t_me), device_id_type=MESH).wait_recv()
    each(ep - 1, back_arrived)

    def sent1(i):
        d = i + 1
        stage1(d).wait_send()
        gate_ep(d).wait_send()
        dx_ep(d).wait_send()
    each(ep - 1, sent1)

    def sent2(d):
        for copy in to_peers(d):
            copy.wait_send()
        for _, _, copy in relays(d):
            copy.wait_send()
        for k in range(1, nx):
            dx_x(k, d).wait_send()
    each(ep, sent2)
    each(nx, lambda k: dx_partner(k).wait_send())
    each(tp - 1, lambda i: gate_tp(i).wait_send())


def fast_kernel(
    ep, tp, cap,
    tok_ref, cot_ref, gid_ref, wid_ref, gw_ref, wg_ref, wu_ref, wd_ref,
    place_ref, back, gate_back, vwg, vwu, vwd,
    gid, wid, gw, src, tok_all, cot_all, placed, rows_in, wg, wu, wd,
    acc, gate_b, up_b, act_c, prod_hi, prod_lo, c_out, c_in,
    to_partner, from_partner, dx_acc, dx_far, to_x, from_x, to_ep, gate_in, gate_sum,
    load_sem, send1, recv_rows, send_p, send_x, send_r, c_send, c_recv,
    dxp_send, dxp_recv, dxx_send, dxx_recv, dxe_send, dxe_recv,
    gt_send, gt_recv, ge_send, ge_recv,
):
    e_me = lax.axis_index("ep")
    t_me = lax.axis_index("tp")
    core = lax.rem(t_me, 2)
    x_me = lax.div(t_me, 2)
    x_other = 1 - x_me
    partner = 2 * x_me + 1 - core
    cross = 2 * x_other + 1 - core
    beyond = 2 * x_other + core
    lanes = gate_back.shape[2]
    tok_rows, width = tok_ref.shape
    cs = width // tp
    slots = ep * cap
    experts = wg.shape[0]
    bf16 = jnp.bfloat16

    barrier = pltpu.get_barrier_semaphore()
    for i in range(ep - 1):
        pl.semaphore_signal(
            barrier, inc=1, device_id=(lax.rem(e_me + 1 + i, ep), partner), device_id_type=MESH)
    for i in range(tp - 1):
        pl.semaphore_signal(
            barrier, inc=1, device_id=(e_me, lax.rem(t_me + 1 + i, tp)), device_id_type=MESH)

    my_cols = pl.ds(pl.multiple_of(t_me * cs, LANES), cs)
    loads = [pltpu.make_async_copy(a, b, load_sem.at[i]) for i, (a, b) in enumerate((
        (gid_ref, gid), (wid_ref, wid), (gw_ref, gw),
        (tok_ref.at[:, my_cols], src.at[:, pl.ds(0, cs)]),
        (cot_ref.at[:, my_cols], src.at[:, pl.ds(cs, cs)]),
        (tok_ref, tok_all), (cot_ref, cot_all),
        (wg_ref, wg), (wu_ref, wu), (wd_ref, wd),
    ))]
    for load in loads[:5]:
        load.start()
    earlier = (
        lax.broadcasted_iota(jnp.int32, (tok_rows, tok_rows), 0)
        < lax.broadcasted_iota(jnp.int32, (tok_rows, tok_rows), 1)
    ).astype(jnp.float32).astype(bf16)
    slot_row = lax.broadcasted_iota(jnp.int32, (slots, tok_rows), 0)
    for load in loads[:3]:
        load.wait()

    group = gid[...]
    groups = -(-ep // 16) * 16
    in_group = (
        lax.broadcasted_iota(jnp.int32, (groups, tok_rows), 0) == group
    ).astype(jnp.float32)
    before = dot(in_group.astype(bf16), earlier)
    rank = jnp.sum(before * in_group, axis=0, keepdims=True).astype(jnp.int32)
    place = (slot_row == group * cap + rank).astype(jnp.float32).astype(bf16)
    place_ref[0] = place
    loads[3].wait()
    placed[:, pl.ds(0, cs)] = dot(place, src[:, pl.ds(0, cs)]).astype(bf16)
    loads[4].wait()
    placed[:, pl.ds(cs, cs)] = dot(place, src[:, pl.ds(cs, cs)]).astype(bf16)
    for load in loads[5:]:
        load.start()

    def xor(d):
        value, bit = 0, 1
        while bit < ep:
            value = value + (e_me // bit + d // bit) % 2 * bit
            bit *= 2
        return value

    def block(e):
        return pl.ds(aligned(e * cap, 16), cap)

    def tile_of(e):
        return e * cap // lanes

    pl.semaphore_wait(barrier, ep + tp - 2)

    def send_rows(d):
        g = xor(d)
        return pltpu.make_async_remote_copy(
            src_ref=placed.at[block(g)], dst_ref=rows_in.at[t_me, block(e_me)],
            send_sem=send1.at[d], recv_sem=recv_rows.at[t_me, e_me],
            device_id=(g, partner), device_id_type=MESH)

    def send_c(d):
        g = xor(d)
        return pltpu.make_async_remote_copy(
            src_ref=c_out.at[tile_of(g)], dst_ref=c_in.at[e_me],
            send_sem=c_send.at[d], recv_sem=c_recv.at[e_me],
            device_id=(g, partner), device_id_type=MESH)

    others = list(range(1, ep))
    for d in others[ep // 2 - 2::-1] + others[:ep // 2 - 2:-1]:
        send_rows(d).start()
    lane_row = lax.broadcasted_iota(jnp.int32, (16, tok_rows), 0)
    weights = gw[...].astype(jnp.float32)
    comb = jnp.zeros((16, tok_rows), jnp.float32)
    for k in range(weights.shape[0]):
        comb = comb + jnp.where(lane_row == wid[k : k + 1, :], weights[k : k + 1, :], 0.0)
    c_rows = dot(comb.astype(bf16), place, NT)
    for i in range(slots // lanes):
        c_out[i] = c_rows[:experts, i * lanes : (i + 1) * lanes]
    for d in others:
        send_c(d).start()

    def arrived(q, d):
        e = xor(d)
        part = rows_in.at[q, block(e)]
        pltpu.make_async_remote_copy(
            src_ref=part, dst_ref=part, send_sem=send1.at[0], recv_sem=recv_rows.at[q, e],
            device_id=(e_me, partner), device_id_type=MESH).wait_recv()

    def pass_on(q, d, sem, device):
        e = xor(d)
        part = rows_in.at[q, block(e)]
        return pltpu.make_async_remote_copy(
            src_ref=part, dst_ref=part, send_sem=sem.at[d], recv_sem=recv_rows.at[q, e],
            device_id=(e_me, device), device_id_type=MESH)

    def to_chips(ds):
        for d in ds:
            arrived(partner, d)
            pass_on(partner, d, send_x, cross).start()
            pass_on(partner, d, send_p, partner).start()

    def relay(ds):
        for d in ds:
            arrived(beyond, d)
            pass_on(beyond, d, send_r, partner).start()

    def wait_rows(q, ds):
        for d in ds:
            arrived(q, d)

    loads[5].wait()
    loads[6].wait()
    own = place_ref[0, block(e_me), :]
    own_x = dot(own, tok_all[...]).astype(bf16)
    own_y = dot(own, cot_all[...]).astype(bf16)
    for q in range(tp):
        rows_in[q, block(e_me), pl.ds(0, cs)] = own_x[:, q * cs : (q + 1) * cs]
        rows_in[q, block(e_me), pl.ds(cs, cs)] = own_y[:, q * cs : (q + 1) * cs]
    c_in[e_me] = c_out[tile_of(e_me)]
    place_ref[1] = (slot_row == e_me * cap % lanes + rank).astype(jnp.float32).astype(bf16)

    def chunk_of(d, n):
        first = xor(d)
        first = first - lax.rem(first, n)
        return first, n, pl.ds(pl.multiple_of(first * cap, cap), n * cap)

    def share(q):
        return pl.ds(aligned(q * cs, LANES), cs)

    def lhs(x, rows, first):
        return jnp.concatenate(
            [rows_in[2 * x + i, rows, pl.ds(first, cs)] for i in range(2)], axis=1)

    def half(chunk, x, keep):
        rows = chunk[2]
        xs, ys = lhs(x, rows, 0), lhs(x, rows, cs)
        cols = pl.ds(pl.multiple_of(x * 2 * cs, LANES), 2 * cs)
        out = []
        for e in range(experts):
            values = (dot(xs, wg[e, cols, :]), dot(xs, wu[e, cols, :]), dot(ys, wd[e, :, cols], NT))
            if keep:
                for n, value in enumerate(values):
                    acc[e, n, rows, :] = value
            out.append(values)
        return out

    def first_half(chunk):
        half(chunk, x_me, True)

    lane = lax.broadcasted_iota(jnp.int32, (cap, lanes), 1)
    lane = lane - lax.broadcasted_iota(jnp.int32, (cap, lanes), 0)
    my_lane = lane == lax.rem(e_me * cap, lanes)

    def second_half(chunk):
        first, n, rows = chunk
        sums = half(chunk, x_other, False)
        for e in range(experts):
            pre_gate, pre_up, dy_down = (acc[e, m, rows, :] + sums[e][m] for m in range(3))
            c = jnp.concatenate([
                jnp.sum(jnp.where(my_lane, c_in[first + i, e : e + 1, :], 0.0), axis=1, keepdims=True)
                for i in range(n)], axis=0)
            sig = jax.nn.sigmoid(pre_gate)
            silu = pre_gate * sig
            act = silu * pre_up
            prod = act.astype(bf16).astype(jnp.float32) * dy_down
            act_grad = c * dy_down
            act_c[e, rows, :] = (c * act).astype(bf16)
            gate_b[e, rows, :] = (act_grad * pre_up * sig * (1.0 + pre_gate * (1.0 - sig))).astype(bf16)
            up_b[e, rows, :] = (act_grad * silu).astype(bf16)
            high = prod.astype(bf16)
            prod_hi[e, rows, :] = high
            prod_lo[e, rows, :] = (prod - high.astype(jnp.float32)).astype(bf16)

    def dx_of(chunk, q, n):
        rows, total = chunk[2], None
        cols = pl.ds(pl.multiple_of(q * cs, LANES), n * cs)
        for e in range(experts):
            part = dot(gate_b[e, rows, :], wg[e, cols, :], NT)
            part = part + dot(up_b[e, rows, :], wu[e, cols, :], NT)
            total = part if total is None else total + part
        return total

    def dx_partner(k, i, chunk):
        return pltpu.make_async_remote_copy(
            src_ref=to_partner.at[k, chunk[2]], dst_ref=from_partner.at[k, chunk[2]],
            send_sem=dxp_send.at[k, i], recv_sem=dxp_recv.at[k, i],
            device_id=(e_me, partner), device_id_type=MESH)

    def dx_x(d):
        e = xor(d)
        return pltpu.make_async_remote_copy(
            src_ref=to_x.at[block(e)], dst_ref=from_x.at[block(e)],
            send_sem=dxx_send.at[d], recv_sem=dxx_recv.at[d],
            device_id=(e_me, cross), device_id_type=MESH)

    def dx_first(i, chunk):
        rows = chunk[2]
        to_partner[0, rows, :] = dx_of(chunk, cross, 1).astype(bf16)
        dx_partner(0, i, chunk).start()

    def dx_rest(i, chunk):
        rows = chunk[2]
        dx_far[rows, :] = dx_of(chunk, beyond, 1)
        both = dx_of(chunk, 2 * x_me, 2)
        low, high = both[:, :cs], both[:, cs:]
        to_partner[1, rows, :] = jnp.where(core == 0, low, high).astype(bf16)
        dx_partner(1, i, chunk).start()
        dx_acc[rows, :] = jnp.where(core == 0, high, low)

    def dx_over(i, chunk, ds):
        dx_partner(0, i, chunk).wait_recv()
        for d in ds:
            rows = block(xor(d))
            to_x[rows, :] = (dx_far[rows, :] + from_partner[0, rows, :].astype(jnp.float32)).astype(bf16)
            dx_x(d).start()

    def dx_ep(d):
        g = xor(d)
        return pltpu.make_async_remote_copy(
            src_ref=to_ep.at[block(g)], dst_ref=back.at[block(e_me)],
            send_sem=dxe_send.at[d], recv_sem=dxe_recv.at[e_me],
            device_id=(g, partner), device_id_type=MESH)

    def own_ready(i, chunk):
        dx_partner(1, i, chunk).wait_recv()

    def send_back(ds):
        for d in ds:
            rows = block(xor(d))
            dx_x(d).wait_recv()
            value = dx_acc[rows, :] + from_partner[1, rows, :].astype(jnp.float32)
            to_ep[rows, :] = (value + from_x[rows, :].astype(jnp.float32)).astype(bf16)
            dx_ep(d).start()

    def gate_tp(i):
        return pltpu.make_async_remote_copy(
            src_ref=gate_in.at[t_me], dst_ref=gate_in.at[t_me],
            send_sem=gt_send.at[i], recv_sem=gt_recv.at[t_me],
            device_id=(e_me, lax.rem(t_me + 1 + i, tp)), device_id_type=MESH)

    def gate_ep(d):
        g = xor(d)
        return pltpu.make_async_remote_copy(
            src_ref=gate_sum.at[tile_of(g)], dst_ref=gate_back.at[e_me],
            send_sem=ge_send.at[d], recv_sem=ge_recv.at[e_me],
            device_id=(g, partner), device_id_type=MESH)

    def gates():
        row8 = lax.broadcasted_iota(jnp.int32, (8, slots), 0)
        ones = jnp.ones((8, prod_hi.shape[2]), bf16)
        value = jnp.zeros((8, slots), jnp.float32)
        for e in range(experts):
            total = dot(ones, prod_hi[e], NT) + dot(ones, prod_lo[e], NT)
            value = value + jnp.where(row8 == e, total, 0.0)
        gate_in[t_me] = value[:experts]
        for i in range(tp - 1):
            gate_tp(i).start()

    def gates_on():
        for i in range(tp - 1):
            q = lax.rem(t_me + 1 + i, tp)
            pltpu.make_async_remote_copy(
                src_ref=gate_in.at[q], dst_ref=gate_in.at[q],
                send_sem=gt_send.at[i], recv_sem=gt_recv.at[q],
                device_id=(e_me, q), device_id_type=MESH).wait_recv()
        total = gate_in[0]
        for q in range(1, tp):
            total = total + gate_in[q]
        for i in range(slots // lanes):
            gate_sum[i] = total[:, i * lanes : (i + 1) * lanes]
        gate_back[e_me] = gate_sum[tile_of(e_me)]
        for d in others:
            gate_ep(d).start()

    def weight_grads(q):
        x_t = rows_in[q, :, pl.ds(0, cs)].T
        yq = rows_in[q, :, pl.ds(cs, cs)]
        for e in range(experts):
            vwg[e, share(q), :] = dot(x_t, gate_b[e]).astype(bf16)
            vwu[e, share(q), :] = dot(x_t, up_b[e]).astype(bf16)
            vwd[e, :, share(q)] = dot(act_c[e], yq, TN).astype(bf16)

    near = others[ep // 2 - 2::-1]
    far_b = others[:-1 - ep // 4:-1]
    far_c = others[-1 - ep // 4:ep // 2 - 2:-1]
    far = far_b + far_c
    a, f = chunk_of(0, ep // 2), chunk_of(ep // 2, ep // 2)
    b, c = chunk_of(far_b[0], ep // 4), chunk_of(far_c[0], ep // 4)

    def c_arrived(ds):
        for d in ds:
            e = xor(d)
            pltpu.make_async_remote_copy(
                src_ref=c_out.at[0], dst_ref=c_in.at[e], send_sem=c_send.at[0],
                recv_sem=c_recv.at[e], device_id=(e_me, partner), device_id_type=MESH).wait_recv()

    to_chips(near)
    for load in loads[7:]:
        load.wait()
    wait_rows(t_me, near)
    first_half(a)
    to_chips(far_b)
    relay(near)
    wait_rows(cross, near)
    c_arrived(near)
    second_half(a)
    to_chips(far_c[:1])
    dx_first(0, a)
    to_chips(far_c[1:])
    relay(far_b)
    dx_rest(0, a)
    wait_rows(t_me, far)
    first_half(f)
    wait_rows(cross, far_b)
    c_arrived(far)
    second_half(b)
    relay(far_c)
    dx_first(1, b)
    dx_rest(1, b)
    dx_over(1, b, far_b)
    dx_over(0, a, [0] + near)
    wait_rows(cross, far_c)
    second_half(c)
    dx_first(2, c)
    gates()
    dx_rest(2, c)
    dx_over(2, c, far_c)
    own_ready(1, b)
    send_back(far_b)
    gates_on()
    weight_grads(0)
    own_ready(0, a)
    own_ready(2, c)
    send_back(far_c)
    send_back(near + [0])
    weight_grads(1)
    weight_grads(2)
    weight_grads(3)

    def returned(d):
        g = xor(d)
        pltpu.make_async_remote_copy(
            src_ref=gate_sum.at[0], dst_ref=gate_back.at[g],
            send_sem=ge_send.at[0], recv_sem=ge_recv.at[g],
            device_id=(g, partner), device_id_type=MESH).wait_recv()

    def rows_back(d):
        g = xor(d)
        pltpu.make_async_remote_copy(
            src_ref=to_ep.at[block(g)], dst_ref=back.at[block(g)],
            send_sem=dxe_send.at[0], recv_sem=dxe_recv.at[g],
            device_id=(g, partner), device_id_type=MESH).wait_recv()

    for d in others:
        returned(d)
    for d in range(ep):
        rows_back(d)
    for d in range(ep):
        dx_x(d).wait_send()
        dx_ep(d).wait_send()
    for d in others:
        send_rows(d).wait_send()
        send_c(d).wait_send()
        pass_on(partner, d, send_x, cross).wait_send()
        pass_on(partner, d, send_p, partner).wait_send()
        pass_on(beyond, d, send_r, partner).wait_send()
        gate_ep(d).wait_send()
    for i, chunk in enumerate((a, b, c)):
        for k in range(2):
            dx_partner(k, i, chunk).wait_send()
    for i in range(tp - 1):
        gate_tp(i).wait_send()


def finish(
    place_ref, back, gate_back, vwg, vwu, vwd, gid_ref, wid_ref,
    dtok_ref, dgate_ref, gwg_ref, gwu_ref, gwd_ref, dtok, dgate, sem,
):
    copies = []
    for a, b in ((vwg, gwg_ref), (vwu, gwu_ref), (vwd, gwd_ref)):
        experts, rows, _ = a.shape
        for e in range(experts):
            for half in range(2):
                part = pl.ds(half * (rows // 2), rows // 2)
                copies.append(pltpu.make_async_copy(
                    a.at[e, part], b.at[e, part], sem.at[2 + len(copies)]))
    for copy in copies:
        copy.start()
    ep, per, slots = gate_back.shape
    tok_rows = place_ref.shape[2]
    dtok[...] = dot(place_ref[0], back[...], TN).astype(jnp.bfloat16)
    copies.append(pltpu.make_async_copy(dtok, dtok_ref, sem.at[0]))
    copies[-1].start()
    sums = jnp.concatenate([gate_back[e] for e in range(ep)], axis=0)
    high = sums.astype(jnp.bfloat16)
    low = (sums - high.astype(jnp.float32)).astype(jnp.bfloat16)
    pick = place_ref[1, :slots, :]
    dense = dot(high, pick) + dot(low, pick)
    row = lax.broadcasted_iota(jnp.int32, (ep * per, tok_rows), 0)
    for k in range(wid_ref.shape[0]):
        wanted = row == gid_ref[...] * per + wid_ref[k : k + 1, :]
        dgate[k : k + 1, :] = jnp.sum(jnp.where(wanted, dense, 0.0), axis=0, keepdims=True)
    copies.append(pltpu.make_async_copy(dgate, dgate_ref, sem.at[1]))
    copies[-1].start()
    for copy in copies:
        copy.wait()


def on_device(tokens, cotangent, group_ids, within_ids, gate_weights, w_gate, w_up, w_down):
    ep = lax.axis_size("ep")
    tp = lax.axis_size("tp")
    tok_rows, width = tokens.shape
    experts, _, ff = w_gate.shape
    cap = (3 * tok_rows + 2 * ep - 1) // (2 * ep)
    cap = -(-cap // 16) * 16
    slots = ep * cap
    gate_lanes = LANES if LANES % cap == 0 and slots % LANES == 0 else slots
    cs = width // tp
    nx = tp // 2
    bf16, f32 = jnp.bfloat16, jnp.float32
    dma = pltpu.SemaphoreType.DMA
    hbm = pl.BlockSpec(memory_space=pltpu.HBM)
    vmem = pl.BlockSpec(memory_space=pltpu.VMEM)
    scratch = [
        pltpu.VMEM((tok_rows, 2 * cs), bf16),
        pltpu.VMEM((slots, 2 * cs + LANES), bf16),
        pltpu.VMEM((tp, slots, 2 * cs + LANES), bf16),
        pltpu.VMEM(w_gate.shape, bf16),
        pltpu.VMEM(w_up.shape, bf16),
        pltpu.VMEM(w_down.shape, bf16),
        pltpu.VMEM((experts, 3, slots, ff), f32),
        pltpu.VMEM((experts, slots, ff), bf16),
        pltpu.VMEM((experts, slots, ff), bf16),
        pltpu.VMEM((experts, slots, ff), bf16),
        pltpu.VMEM((nx, slots, cs), bf16),
        pltpu.VMEM((nx, slots, cs), bf16),
        pltpu.VMEM((slots, cs), f32),
        pltpu.VMEM((nx - 1, slots, cs), bf16),
        pltpu.VMEM((nx - 1, slots, cs), bf16),
        pltpu.VMEM((slots, cs), bf16),
        pltpu.VMEM((tp, 8, slots), f32),
        pltpu.VMEM((8, slots), f32),
        dma((5,)), dma((1,)), dma((ep,)), dma((tp, ep)),
        dma((nx - 1, ep)), dma((ep,)), dma((nx - 1, ep)),
        dma((nx,)), dma((nx,)), dma((nx - 1, ep)), dma((nx - 1, ep)), dma((ep,)), dma((ep,)),
        dma((tp,)), dma((tp,)), dma((ep,)), dma((ep,)),
    ]
    gid, wid, gw = group_ids.T, within_ids.T, gate_weights.T
    body, per, small = kernel, 8, vmem
    if ep == 8 and tp == 4 and gate_lanes == LANES:
        body, per, small = fast_kernel, experts, hbm
        scratch = [
            pltpu.VMEM(gid.shape, jnp.int32),
            pltpu.VMEM(wid.shape, jnp.int32),
            pltpu.VMEM(gw.shape, bf16),
            pltpu.VMEM((tok_rows, 2 * cs), bf16),
            pltpu.VMEM((tok_rows, width), bf16),
            pltpu.VMEM((tok_rows, width), bf16),
            pltpu.VMEM((slots, 2 * cs), bf16),
            pltpu.VMEM((tp, slots, 2 * cs), bf16),
            pltpu.VMEM(w_gate.shape, bf16),
            pltpu.VMEM(w_up.shape, bf16),
            pltpu.VMEM(w_down.shape, bf16),
            pltpu.VMEM((experts, 3, slots, ff), f32),
            pltpu.VMEM((experts, slots, ff), bf16),
            pltpu.VMEM((experts, slots, ff), bf16),
            pltpu.VMEM((experts, slots, ff), bf16),
            pltpu.VMEM((experts, slots, ff), bf16),
            pltpu.VMEM((experts, slots, ff), bf16),
            pltpu.VMEM((slots // gate_lanes, experts, gate_lanes), f32),
            pltpu.VMEM((ep, experts, gate_lanes), f32),
            pltpu.VMEM((2, slots, cs), bf16),
            pltpu.VMEM((2, slots, cs), bf16),
            pltpu.VMEM((slots, cs), f32),
            pltpu.VMEM((slots, cs), f32),
            pltpu.VMEM((slots, cs), bf16),
            pltpu.VMEM((slots, cs), bf16),
            pltpu.VMEM((slots, cs), bf16),
            pltpu.VMEM((tp, experts, slots), f32),
            pltpu.VMEM((slots // gate_lanes, experts, gate_lanes), f32),
            dma((10,)), dma((ep,)), dma((tp, ep)), dma((ep,)), dma((ep,)), dma((ep,)),
            dma((ep,)), dma((ep,)), dma((2, 3)), dma((2, 3)), dma((ep,)), dma((ep,)),
            dma((ep,)), dma((ep,)), dma((tp,)), dma((tp,)), dma((ep,)), dma((ep,)),
        ]
    kept = pl.pallas_call(
        functools.partial(body, ep, tp, cap),
        out_shape=(
            pltpu.VMEM((2, slots, tok_rows), bf16),
            pltpu.VMEM((slots, cs), bf16),
            pltpu.VMEM((ep, per, gate_lanes), f32),
            pltpu.VMEM(w_gate.shape, bf16),
            pltpu.VMEM(w_up.shape, bf16),
            pltpu.VMEM(w_down.shape, bf16),
        ),
        in_specs=[hbm, hbm, small, small, small, hbm, hbm, hbm],
        out_specs=(vmem,) * 6,
        scratch_shapes=scratch,
        compiler_params=pltpu.CompilerParams(
            collective_id=0, has_side_effects=True, vmem_limit_bytes=57 * 1024 * 1024),
    )(tokens, cotangent, gid, wid, gw, w_gate, w_up, w_down)
    dtok, dgate, gwg, gwu, gwd = pl.pallas_call(
        finish,
        out_shape=(
            jax.ShapeDtypeStruct((tok_rows, cs), bf16),
            jax.ShapeDtypeStruct(wid.shape, f32),
            jax.ShapeDtypeStruct(w_gate.shape, bf16),
            jax.ShapeDtypeStruct(w_up.shape, bf16),
            jax.ShapeDtypeStruct(w_down.shape, bf16),
        ),
        in_specs=[vmem] * 8,
        out_specs=(hbm,) * 5,
        scratch_shapes=[
            pltpu.VMEM((tok_rows, cs), bf16),
            pltpu.VMEM(wid.shape, f32),
            dma((2 + 6 * experts,)),
        ],
        compiler_params=pltpu.CompilerParams(vmem_limit_bytes=12 * 1024 * 1024),
    )(*kept, gid, wid)
    return dtok, dgate.T, gwg, gwu, gwd


def solution(mesh):
    in_specs = (
        P("ep", None),
        P("ep", None),
        P("ep", None),
        P("ep", None),
        P("ep", None),
        P("ep", None, "tp"),
        P("ep", None, "tp"),
        P("ep", "tp", None),
    )
    out_specs = (
        P("ep", "tp"),
        P("ep", None),
        P("ep", None, "tp"),
        P("ep", None, "tp"),
        P("ep", "tp", None),
    )
    return jax.shard_map(
        on_device, mesh=mesh, in_specs=in_specs, out_specs=out_specs, check_vma=False
    )
```

```python
import functools

import jax
import jax.numpy as jnp
from jax import lax
from jax.experimental import pallas as pl
from jax.experimental.pallas import tpu as pltpu
from jax.sharding import PartitionSpec as P

MESH = pl.DeviceIdType.MESH
LANES = 128
NT = (((1,), (1,)), ((), ()))
TN = (((0,), (0,)), ((), ()))
NN = (((1,), (0,)), ((), ()))


def dot(a, b, dims=NN):
    return lax.dot_general(a, b, dims, preferred_element_type=jnp.float32)


def each(count, body):
    if count <= 8:
        for i in range(count):
            body(i)
    else:
        lax.fori_loop(0, count, lambda i, c: (body(i), c)[1], 0)


def aligned(value, step):
    return value if isinstance(value, int) else pl.multiple_of(value, step)


def kernel(
    ep, tp, cap,
    tok_ref, cot_ref, gid_ref, wid_ref, gw_ref, wg_ref, wu_ref, wd_ref,
    place_ref, back, gate_back, vwg, vwu, vwd,
    src, placed, rows_in, wg, wu, wd, acc, gate_b, up_b, act_c,
    to_partner, from_partner, dx_acc, to_x, from_x, to_ep,
    gate_in, gate_sum,
    load_sem, own_sem, send1, recv_rows, send_x, send_p, send_p2,
    dxp_send, dxp_recv, dxx_send, dxx_recv, dxe_send, dxe_recv,
    gt_send, gt_recv, ge_send, ge_recv,
):
    e_me = lax.axis_index("ep")
    t_me = lax.axis_index("tp")
    core = lax.rem(t_me, 2)
    x_me = lax.div(t_me, 2)
    partner = t_me + 1 - 2 * core
    nx = tp // 2
    gate_lanes = gate_back.shape[2]
    tok_rows, width = tok_ref.shape
    cs = width // tp
    slots = ep * cap
    experts = wg.shape[0]
    bf16 = jnp.bfloat16

    barrier = pltpu.get_barrier_semaphore()
    each(ep - 1, lambda i: pl.semaphore_signal(
        barrier, inc=1, device_id=(lax.rem(e_me + 1 + i, ep), t_me), device_id_type=MESH))
    each(tp - 1, lambda i: pl.semaphore_signal(
        barrier, inc=1, device_id=(e_me, lax.rem(t_me + 1 + i, tp)), device_id_type=MESH))

    my_cols = pl.ds(pl.multiple_of(t_me * cs, LANES), cs)
    loads = [
        pltpu.make_async_copy(tok_ref.at[:, my_cols], src.at[:, pl.ds(0, cs)], load_sem.at[0]),
        pltpu.make_async_copy(cot_ref.at[:, my_cols], src.at[:, pl.ds(cs, cs)], load_sem.at[1]),
        pltpu.make_async_copy(wg_ref, wg, load_sem.at[2]),
        pltpu.make_async_copy(wu_ref, wu, load_sem.at[3]),
        pltpu.make_async_copy(wd_ref, wd, load_sem.at[4]),
    ]
    for load in loads[:2]:
        load.start()

    group = gid_ref[...]
    groups = -(-ep // 16) * 16
    in_group = (
        lax.broadcasted_iota(jnp.int32, (groups, tok_rows), 0) == group
    ).astype(jnp.float32)
    earlier = (
        lax.broadcasted_iota(jnp.int32, (tok_rows, tok_rows), 0)
        < lax.broadcasted_iota(jnp.int32, (tok_rows, tok_rows), 1)
    ).astype(jnp.float32).astype(bf16)
    before = dot(in_group.astype(bf16), earlier)
    rank = jnp.sum(before * in_group, axis=0, keepdims=True).astype(jnp.int32)
    slot_row = lax.broadcasted_iota(jnp.int32, (slots, tok_rows), 0)
    place = (slot_row == group * cap + rank).astype(jnp.float32).astype(bf16)
    place_ref[0] = place
    place_ref[1] = (slot_row == e_me * cap % gate_lanes + rank).astype(jnp.float32).astype(bf16)
    lane_row = lax.broadcasted_iota(jnp.int32, (LANES, tok_rows), 0)
    weights = gw_ref[...].astype(jnp.float32)
    comb = jnp.zeros((LANES, tok_rows), jnp.float32)
    for k in range(weights.shape[0]):
        comb = comb + jnp.where(lane_row == wid_ref[k : k + 1, :], weights[k : k + 1, :], 0.0)
    placed[:, pl.ds(2 * cs, LANES)] = dot(place, comb.astype(bf16), NT).astype(bf16)
    loads[0].wait()
    placed[:, pl.ds(0, cs)] = dot(place, src[:, pl.ds(0, cs)]).astype(bf16)
    loads[1].wait()
    for load in loads[2:]:
        load.start()
    placed[:, pl.ds(cs, cs)] = dot(place, src[:, pl.ds(cs, cs)]).astype(bf16)

    pl.semaphore_wait(barrier, ep + tp - 2)

    def xor(d):
        value, bit = 0, 1
        while bit < ep:
            value = value + (e_me // bit + d // bit) % 2 * bit
            bit *= 2
        return value

    def target(d):
        return xor(d) if ep & (ep - 1) == 0 else lax.rem(e_me + d, ep)

    def source(d):
        return xor(d) if ep & (ep - 1) == 0 else lax.rem(e_me - d + ep, ep)

    def block(e):
        return pl.ds(aligned(e * cap, 16), cap)

    distances = list(range(ep))
    def stage1(d):
        g = target(d)
        return pltpu.make_async_remote_copy(
            src_ref=placed.at[block(g)], dst_ref=rows_in.at[t_me, block(e_me)],
            send_sem=send1.at[d], recv_sem=recv_rows.at[t_me, e_me],
            device_id=(g, t_me), device_id_type=MESH)

    own = pltpu.make_async_copy(
        placed.at[block(e_me)], rows_in.at[t_me, block(e_me)], own_sem.at[0])
    own.start()
    if ep <= 8:
        for d in distances[1:]:
            stage1(d).start()
    else:
        each(ep - 1, lambda i: stage1(i + 1).start())

    def arrived(q, e, cols):
        part = rows_in.at[q, block(e), pl.ds(0, cols)]
        pltpu.make_async_remote_copy(
            src_ref=part, dst_ref=part, send_sem=send1.at[0], recv_sem=recv_rows.at[q, e],
            device_id=(e_me, partner), device_id_type=MESH).wait_recv()

    def forward(q, e, sem, target):
        part = rows_in.at[q, block(e), pl.ds(0, 2 * cs)]
        return pltpu.make_async_remote_copy(
            src_ref=part, dst_ref=part, send_sem=sem, recv_sem=recv_rows.at[q, e],
            device_id=(e_me, target), device_id_type=MESH)

    def x_peer(k):
        return lax.rem(x_me + k, nx) * 2 + core

    def to_peers(d):
        e = source(d)
        copies = [forward(t_me, e, send_x.at[k - 1, d], x_peer(k)) for k in range(1, nx)]
        return copies + [forward(t_me, e, send_p.at[d], partner)]

    def stage2(d):
        for copy in to_peers(d):
            copy.start()

    def relays(d):
        e = source(d)
        return [(x_peer(k), e, forward(x_peer(k), e, send_p2.at[k - 1, d], partner))
                for k in range(1, nx)]

    def stage3(d):
        for q, e, copy in relays(d):
            arrived(q, e, 2 * cs)
            copy.start()

    own.wait()
    stage2(0)
    if ep <= 8:
        for i, d in enumerate(distances[1:]):
            arrived(t_me, source(d), 2 * cs + LANES)
            stage2(d)
    else:
        def later(i):
            arrived(t_me, source(i + 1), 2 * cs + LANES)
            stage2(i + 1)
        each(ep - 1, later)

    for load in loads[2:]:
        load.wait()

    def share(q):
        return pl.ds(aligned(q * cs, LANES), cs)

    def hidden(q, first):
        xq = rows_in[q, :, pl.ds(0, cs)]
        yq = rows_in[q, :, pl.ds(cs, cs)]
        for e in range(experts):
            for n, value in enumerate((
                dot(xq, wg[e, share(q), :]),
                dot(xq, wu[e, share(q), :]),
                dot(yq, wd[e, :, share(q)], NT),
            )):
                acc[e, n] = value if first else acc[e, n] + value

    def all_arrived(q):
        each(ep, lambda e: arrived(q, e, 2 * cs))

    hidden(t_me, True)
    if ep <= 8:
        for d in distances:
            stage3(d)
    else:
        each(ep, stage3)
    all_arrived(partner)
    hidden(partner, False)

    def x_quarters(k):
        hidden(x_peer(k), False)
        other = lax.rem(x_me + k, nx) * 2 + 1 - core
        all_arrived(other)
        hidden(other, False)
    each(nx - 1, lambda i: x_quarters(i + 1))

    row8 = lax.broadcasted_iota(jnp.int32, (8, slots), 0)
    gates = jnp.zeros((8, slots), jnp.float32)
    for e in range(experts):
        pre_gate, pre_up, dy_down = acc[e, 0], acc[e, 1], acc[e, 2]
        c = rows_in[t_me, :, pl.ds(2 * cs, LANES)][:, e : e + 1].astype(jnp.float32)
        sig = jax.nn.sigmoid(pre_gate)
        silu = pre_gate * sig
        act = silu * pre_up
        prod = act.astype(bf16).astype(jnp.float32) * dy_down
        act_grad = c * dy_down
        act_c[e] = (c * act).astype(bf16)
        gate_b[e] = (act_grad * pre_up * sig * (1.0 + pre_gate * (1.0 - sig))).astype(bf16)
        up_b[e] = (act_grad * silu).astype(bf16)
        high = prod.astype(bf16)
        low = (prod - high.astype(jnp.float32)).astype(bf16)
        ones = jnp.ones((8, prod.shape[1]), bf16)
        gates = gates + jnp.where(row8 == e, dot(ones, high, NT) + dot(ones, low, NT), 0.0)
    gate_in[t_me] = gates

    def gate_tp(i):
        return pltpu.make_async_remote_copy(
            src_ref=gate_in.at[t_me], dst_ref=gate_in.at[t_me],
            send_sem=gt_send.at[i], recv_sem=gt_recv.at[t_me],
            device_id=(e_me, lax.rem(t_me + 1 + i, tp)), device_id_type=MESH)

    def dx_of(q):
        total = None
        for e in range(experts):
            part = dot(gate_b[e], wg[e, share(q), :], NT) + dot(up_b[e], wu[e, share(q), :], NT)
            total = part if total is None else total + part
        return total

    def dx_partner(k):
        return pltpu.make_async_remote_copy(
            src_ref=to_partner.at[k], dst_ref=from_partner.at[k],
            send_sem=dxp_send.at[k], recv_sem=dxp_recv.at[k],
            device_id=(e_me, partner), device_id_type=MESH)

    def give_partner(i):
        k = nx - 1 - i
        to_partner[k] = dx_of(lax.rem(x_me + k, nx) * 2 + 1 - core).astype(bf16)
        dx_partner(k).start()

    def dx_x(k, d):
        e = target(d)
        return pltpu.make_async_remote_copy(
            src_ref=to_x.at[k - 1, block(e)], dst_ref=from_x.at[k - 1, block(e)],
            send_sem=dxx_send.at[k - 1, d], recv_sem=dxx_recv.at[k - 1, d],
            device_id=(e_me, x_peer(k)), device_id_type=MESH)

    far = distances[::-1]

    def walk(body):
        if ep <= 8:
            for i, d in enumerate(far):
                body(i, d)
        else:
            each(ep, lambda i: body(i, ep - 1 - i))

    def give_x(k):
        mine = dx_of(x_peer(k))
        dx_partner(k).wait_recv()
        to_x[k - 1] = (mine + from_partner[k].astype(jnp.float32)).astype(bf16)
        walk(lambda i, d: dx_x(k, d).start())
    each(tp - 1, lambda i: gate_tp(i).start())

    def cross(i):
        give_partner(i)
        give_x(nx - 1 - i)
    each(nx - 1, cross)
    give_partner(nx - 1)
    mine = dx_of(t_me)
    dx_partner(0).wait_recv()
    dx_acc[...] = mine + from_partner[0].astype(jnp.float32)

    def gate_tile(e):
        return pl.ds(pl.multiple_of(e * cap // gate_lanes * gate_lanes, LANES), gate_lanes)

    def gate_ep(d):
        return pltpu.make_async_remote_copy(
            src_ref=gate_sum.at[:, gate_tile(target(d))], dst_ref=gate_back.at[e_me],
            send_sem=ge_send.at[d], recv_sem=ge_recv.at[e_me],
            device_id=(target(d), t_me), device_id_type=MESH)

    def gate_wait(i):
        q = lax.rem(t_me + 1 + i, tp)
        pltpu.make_async_remote_copy(
            src_ref=gate_in.at[q], dst_ref=gate_in.at[q],
            send_sem=gt_send.at[i], recv_sem=gt_recv.at[q],
            device_id=(e_me, q), device_id_type=MESH).wait_recv()

    def gates_on():
        each(tp - 1, gate_wait)
        total = gate_in[0]
        for q in range(1, tp):
            total = total + gate_in[q]
        gate_sum[...] = total
        gate_back[e_me] = gate_sum[:, gate_tile(e_me)]
        each(ep - 1, lambda i: gate_ep(i + 1).start())

    def weight_grads(q):
        x_t = rows_in[q, :, pl.ds(0, cs)].T
        yq = rows_in[q, :, pl.ds(cs, cs)]
        for e in range(experts):
            vwg[e, share(q), :] = dot(x_t, gate_b[e]).astype(bf16)
            vwu[e, share(q), :] = dot(x_t, up_b[e]).astype(bf16)
            vwd[e, :, share(q)] = dot(act_c[e], yq, TN).astype(bf16)

    def dx_ep(d):
        g = target(d)
        return pltpu.make_async_remote_copy(
            src_ref=to_ep.at[block(g)], dst_ref=back.at[block(e_me)],
            send_sem=dxe_send.at[d], recv_sem=dxe_recv.at[e_me],
            device_id=(g, t_me), device_id_type=MESH)

    def finish_chunk(d):
        rows = block(target(d))
        value = dx_acc[rows, :]
        for k in range(1, nx):
            dx_x(k, d).wait_recv()
            value = value + from_x[k - 1, rows, :].astype(jnp.float32)
        return value.astype(bf16)

    def chunk(i, d):
        to_ep[block(target(d)), :] = finish_chunk(d)
        dx_ep(d).start()

    if ep <= 8:
        done = 0
        for i, d in enumerate(far[:-1]):
            chunk(i, d)
            if i % 2 == 0 and done < tp:
                weight_grads(done)
                done += 1
            if i == min(2, ep - 2):
                gates_on()
        for q in range(done, tp):
            weight_grads(q)
    else:
        each(ep - 1, lambda i: chunk(i, ep - 1 - i))
        each(tp, weight_grads)
        gates_on()
    back[block(e_me), :] = finish_chunk(0)

    def gate_arrived(i):
        g = lax.rem(e_me + 1 + i, ep)
        pltpu.make_async_remote_copy(
            src_ref=gate_sum.at[:, gate_tile(g)], dst_ref=gate_back.at[g],
            send_sem=ge_send.at[0], recv_sem=ge_recv.at[g],
            device_id=(g, t_me), device_id_type=MESH).wait_recv()
    each(ep - 1, gate_arrived)
    def back_arrived(i):
        g = lax.rem(e_me + 1 + i, ep)
        pltpu.make_async_remote_copy(
            src_ref=to_ep.at[block(g)], dst_ref=back.at[block(g)],
            send_sem=dxe_send.at[0], recv_sem=dxe_recv.at[g],
            device_id=(g, t_me), device_id_type=MESH).wait_recv()
    each(ep - 1, back_arrived)

    def sent1(i):
        d = i + 1
        stage1(d).wait_send()
        gate_ep(d).wait_send()
        dx_ep(d).wait_send()
    each(ep - 1, sent1)

    def sent2(d):
        for copy in to_peers(d):
            copy.wait_send()
        for _, _, copy in relays(d):
            copy.wait_send()
        for k in range(1, nx):
            dx_x(k, d).wait_send()
    each(ep, sent2)
    each(nx, lambda k: dx_partner(k).wait_send())
    each(tp - 1, lambda i: gate_tp(i).wait_send())


def fast_kernel(
    ep, tp, cap,
    tok_ref, cot_ref, gid_ref, wid_ref, gw_ref, wg_ref, wu_ref, wd_ref,
    place_ref, back, gate_back, vwg, vwu, vwd,
    gid, wid, gw, src, tok_all, cot_all, placed, rows_in, wg, wu, wd,
    wide, acc, gate_b, up_b, act_c, prod_hi, prod_lo, c_out, c_in,
    to_partner, from_partner, dx_acc, dx_far, to_x, from_x, to_ep, gate_in, gate_sum,
    load_sem, wide_send, send1, recv_rows, send_p, send_x, send_r, c_send, c_recv,
    dxp_send, dxp_recv, dxx_send, dxx_recv, dxe_send, dxe_recv,
    gt_send, gt_recv, ge_send, ge_recv,
):
    e_me = lax.axis_index("ep")
    t_me = lax.axis_index("tp")
    core = lax.rem(t_me, 2)
    x_me = lax.div(t_me, 2)
    x_other = 1 - x_me
    partner = 2 * x_me + 1 - core
    cross = 2 * x_other + 1 - core
    beyond = 2 * x_other + core
    lanes = gate_back.shape[2]
    tok_rows, width = tok_ref.shape
    cs = width // tp
    slots = ep * cap
    experts = wg.shape[0]
    bf16 = jnp.bfloat16

    barrier = pltpu.get_barrier_semaphore()
    for i in range(ep - 1):
        pl.semaphore_signal(
            barrier, inc=1, device_id=(lax.rem(e_me + 1 + i, ep), partner), device_id_type=MESH)
    for i in range(tp - 1):
        pl.semaphore_signal(
            barrier, inc=1, device_id=(e_me, lax.rem(t_me + 1 + i, tp)), device_id_type=MESH)

    my_cols = pl.ds(pl.multiple_of(t_me * cs, LANES), cs)
    loads = [pltpu.make_async_copy(a, b, load_sem.at[i]) for i, (a, b) in enumerate((
        (gid_ref, gid), (wid_ref, wid), (gw_ref, gw),
        (tok_ref.at[:, my_cols], src.at[:, pl.ds(0, cs)]),
        (cot_ref.at[:, my_cols], src.at[:, pl.ds(cs, cs)]),
        (tok_ref, tok_all), (cot_ref, cot_all),
        (wg_ref, wg), (wu_ref, wu), (wd_ref, wd),
    ))]
    for load in loads[:5]:
        load.start()
    earlier = (
        lax.broadcasted_iota(jnp.int32, (tok_rows, tok_rows), 0)
        < lax.broadcasted_iota(jnp.int32, (tok_rows, tok_rows), 1)
    ).astype(jnp.float32).astype(bf16)
    slot_row = lax.broadcasted_iota(jnp.int32, (slots, tok_rows), 0)
    for load in loads[:3]:
        load.wait()

    group = gid[...]
    groups = -(-ep // 16) * 16
    in_group = (
        lax.broadcasted_iota(jnp.int32, (groups, tok_rows), 0) == group
    ).astype(jnp.float32)
    before = dot(in_group.astype(bf16), earlier)
    rank = jnp.sum(before * in_group, axis=0, keepdims=True).astype(jnp.int32)
    place = (slot_row == group * cap + rank).astype(jnp.float32).astype(bf16)
    place_ref[0] = place
    loads[3].wait()
    placed[:, pl.ds(0, cs)] = dot(place, src[:, pl.ds(0, cs)]).astype(bf16)
    loads[4].wait()
    placed[:, pl.ds(cs, cs)] = dot(place, src[:, pl.ds(cs, cs)]).astype(bf16)
    for load in loads[5:]:
        load.start()

    def xor(d):
        value, bit = 0, 1
        while bit < ep:
            value = value + (e_me // bit + d // bit) % 2 * bit
            bit *= 2
        return value

    def block(e):
        return pl.ds(aligned(e * cap, 16), cap)

    def tile_of(e):
        return e * cap // lanes

    pl.semaphore_wait(barrier, ep + tp - 2)

    def send_rows(d):
        g = xor(d)
        return pltpu.make_async_remote_copy(
            src_ref=placed.at[block(g)], dst_ref=rows_in.at[t_me, block(e_me)],
            send_sem=send1.at[d], recv_sem=recv_rows.at[t_me, e_me],
            device_id=(g, partner), device_id_type=MESH)

    def send_c(d):
        g = xor(d)
        return pltpu.make_async_remote_copy(
            src_ref=c_out.at[tile_of(g)], dst_ref=c_in.at[e_me],
            send_sem=c_send.at[d], recv_sem=c_recv.at[e_me],
            device_id=(g, partner), device_id_type=MESH)

    others = list(range(1, ep))
    def send_wide():
        return pltpu.make_async_remote_copy(
            src_ref=wide, dst_ref=rows_in.at[beyond, block(e_me)],
            send_sem=wide_send.at[0], recv_sem=recv_rows.at[beyond, e_me],
            device_id=(xor(1), partner), device_id_type=MESH)

    for d in others[1:ep // 2 - 1] + others[:1] + others[:ep // 2 - 2:-1]:
        send_rows(d).start()
    loads[5].wait()
    loads[6].wait()
    beside = place_ref[0, block(xor(1)), :]
    far_cols = pl.ds(pl.multiple_of(beyond * cs, LANES), cs)
    wide[:, pl.ds(0, cs)] = dot(beside, tok_all[:, far_cols]).astype(bf16)
    wide[:, pl.ds(cs, cs)] = dot(beside, cot_all[:, far_cols]).astype(bf16)
    send_wide().start()
    lane_row = lax.broadcasted_iota(jnp.int32, (16, tok_rows), 0)
    weights = gw[...].astype(jnp.float32)
    comb = jnp.zeros((16, tok_rows), jnp.float32)
    for k in range(weights.shape[0]):
        comb = comb + jnp.where(lane_row == wid[k : k + 1, :], weights[k : k + 1, :], 0.0)
    c_rows = dot(comb.astype(bf16), place, NT)
    for i in range(slots // lanes):
        c_out[i] = c_rows[:experts, i * lanes : (i + 1) * lanes]
    for d in others:
        send_c(d).start()

    def arrived(q, d):
        e = xor(d)
        part = rows_in.at[q, block(e)]
        pltpu.make_async_remote_copy(
            src_ref=part, dst_ref=part, send_sem=send1.at[0], recv_sem=recv_rows.at[q, e],
            device_id=(e_me, partner), device_id_type=MESH).wait_recv()

    def pass_on(q, d, sem, device):
        e = xor(d)
        part = rows_in.at[q, block(e)]
        return pltpu.make_async_remote_copy(
            src_ref=part, dst_ref=part, send_sem=sem.at[d], recv_sem=recv_rows.at[q, e],
            device_id=(e_me, device), device_id_type=MESH)

    def to_chips(ds):
        for d in ds:
            arrived(partner, d)
            if d != 1:
                pass_on(partner, d, send_x, cross).start()
            pass_on(partner, d, send_p, partner).start()

    def relayed(d):
        return pass_on(cross if d == 1 else beyond, d, send_r, partner)

    def relay(ds):
        for d in ds:
            arrived(cross if d == 1 else beyond, d)
            relayed(d).start()

    def wait_own(ds):
        for d in ds:
            arrived(t_me, d)

    def wait_last(ds):
        for d in ds:
            arrived(beyond if d == 1 else cross, d)

    own = place_ref[0, block(e_me), :]
    own_x = dot(own, tok_all[...]).astype(bf16)
    own_y = dot(own, cot_all[...]).astype(bf16)
    for q in range(tp):
        rows_in[q, block(e_me), pl.ds(0, cs)] = own_x[:, q * cs : (q + 1) * cs]
        rows_in[q, block(e_me), pl.ds(cs, cs)] = own_y[:, q * cs : (q + 1) * cs]
    c_in[e_me] = c_out[tile_of(e_me)]
    place_ref[1] = (slot_row == e_me * cap % lanes + rank).astype(jnp.float32).astype(bf16)

    def chunk_of(d, n):
        first = xor(d)
        first = first - lax.rem(first, n)
        return first, n, pl.ds(pl.multiple_of(first * cap, cap), n * cap)

    def share(q):
        return pl.ds(aligned(q * cs, LANES), cs)

    def lhs(x, rows, first):
        return jnp.concatenate(
            [rows_in[2 * x + i, rows, pl.ds(first, cs)] for i in range(2)], axis=1)

    def half(chunk, x, keep):
        rows = chunk[2]
        xs, ys = lhs(x, rows, 0), lhs(x, rows, cs)
        cols = pl.ds(pl.multiple_of(x * 2 * cs, LANES), 2 * cs)
        out = []
        for e in range(experts):
            values = (dot(xs, wg[e, cols, :]), dot(xs, wu[e, cols, :]), dot(ys, wd[e, :, cols], NT))
            if keep:
                for n, value in enumerate(values):
                    acc[e, n, rows, :] = value
            out.append(values)
        return out

    alone = pl.when(e_me >= 0)

    def keep_half(chunk):
        half(chunk, x_me, True)

    def first_half(chunk):
        alone(lambda: keep_half(chunk))

    lane = lax.broadcasted_iota(jnp.int32, (cap, lanes), 1)
    lane = lane - lax.broadcasted_iota(jnp.int32, (cap, lanes), 0)
    my_lane = lane == lax.rem(e_me * cap, lanes)

    def second_half(chunk):
        alone(lambda: activations(chunk))

    def activations(chunk):
        first, n, rows = chunk
        sums = half(chunk, x_other, False)
        for e in range(experts):
            pre_gate, pre_up, dy_down = (acc[e, m, rows, :] + sums[e][m] for m in range(3))
            c = jnp.concatenate([
                jnp.sum(jnp.where(my_lane, c_in[first + i, e : e + 1, :], 0.0), axis=1, keepdims=True)
                for i in range(n)], axis=0)
            sig = jax.nn.sigmoid(pre_gate)
            silu = pre_gate * sig
            act = silu * pre_up
            prod = act.astype(bf16).astype(jnp.float32) * dy_down
            act_grad = c * dy_down
            act_c[e, rows, :] = (c * act).astype(bf16)
            gate_b[e, rows, :] = (act_grad * pre_up * sig * (1.0 + pre_gate * (1.0 - sig))).astype(bf16)
            up_b[e, rows, :] = (act_grad * silu).astype(bf16)
            high = prod.astype(bf16)
            prod_hi[e, rows, :] = high
            prod_lo[e, rows, :] = (prod - high.astype(jnp.float32)).astype(bf16)

    def dx_of(chunk, q, n):
        rows, total = chunk[2], None
        cols = pl.ds(pl.multiple_of(q * cs, LANES), n * cs)
        for e in range(experts):
            part = dot(gate_b[e, rows, :], wg[e, cols, :], NT)
            part = part + dot(up_b[e, rows, :], wu[e, cols, :], NT)
            total = part if total is None else total + part
        return total

    def dx_partner(k, i, chunk):
        return pltpu.make_async_remote_copy(
            src_ref=to_partner.at[k, chunk[2]], dst_ref=from_partner.at[k, chunk[2]],
            send_sem=dxp_send.at[k, i], recv_sem=dxp_recv.at[k, i],
            device_id=(e_me, partner), device_id_type=MESH)

    def dx_x(d):
        e = xor(d)
        return pltpu.make_async_remote_copy(
            src_ref=to_x.at[block(e)], dst_ref=from_x.at[block(e)],
            send_sem=dxx_send.at[d], recv_sem=dxx_recv.at[d],
            device_id=(e_me, cross), device_id_type=MESH)

    def dx_first(i, chunk):
        @alone
        def _():
            to_partner[0, chunk[2], :] = dx_of(chunk, cross, 1).astype(bf16)
            dx_partner(0, i, chunk).start()

    def dx_rest(i, chunk):
        @alone
        def _():
            dx_other_chip(chunk)
            dx_my_chip(i, chunk)

    def dx_other_chip(chunk):
        dx_far[chunk[2], :] = dx_of(chunk, beyond, 1)

    def dx_my_chip(i, chunk):
        rows = chunk[2]
        both = dx_of(chunk, 2 * x_me, 2)
        low, high = both[:, :cs], both[:, cs:]
        to_partner[1, rows, :] = jnp.where(core == 0, low, high).astype(bf16)
        dx_partner(1, i, chunk).start()
        dx_acc[rows, :] = jnp.where(core == 0, high, low)

    def dx_over(i, chunk, ds):
        dx_partner(0, i, chunk).wait_recv()
        for d in ds:
            rows = block(xor(d))
            to_x[rows, :] = (dx_far[rows, :] + from_partner[0, rows, :].astype(jnp.float32)).astype(bf16)
            dx_x(d).start()

    def dx_ep(d):
        g = xor(d)
        return pltpu.make_async_remote_copy(
            src_ref=to_ep.at[block(g)], dst_ref=back.at[block(e_me)],
            send_sem=dxe_send.at[d], recv_sem=dxe_recv.at[e_me],
            device_id=(g, partner), device_id_type=MESH)

    def own_ready(i, chunk):
        dx_partner(1, i, chunk).wait_recv()

    def send_back(ds):
        for d in ds:
            rows = block(xor(d))
            dx_x(d).wait_recv()
            value = dx_acc[rows, :] + from_partner[1, rows, :].astype(jnp.float32)
            to_ep[rows, :] = (value + from_x[rows, :].astype(jnp.float32)).astype(bf16)
            dx_ep(d).start()

    def gate_tp(i):
        return pltpu.make_async_remote_copy(
            src_ref=gate_in.at[t_me], dst_ref=gate_in.at[t_me],
            send_sem=gt_send.at[i], recv_sem=gt_recv.at[t_me],
            device_id=(e_me, lax.rem(t_me + 1 + i, tp)), device_id_type=MESH)

    def gate_ep(d):
        g = xor(d)
        return pltpu.make_async_remote_copy(
            src_ref=gate_sum.at[tile_of(g)], dst_ref=gate_back.at[e_me],
            send_sem=ge_send.at[d], recv_sem=ge_recv.at[e_me],
            device_id=(g, partner), device_id_type=MESH)

    def gates():
        alone(gate_sums)

    def gate_sums():
        row8 = lax.broadcasted_iota(jnp.int32, (8, slots), 0)
        ones = jnp.ones((8, prod_hi.shape[2]), bf16)
        value = jnp.zeros((8, slots), jnp.float32)
        for e in range(experts):
            total = dot(ones, prod_hi[e], NT) + dot(ones, prod_lo[e], NT)
            value = value + jnp.where(row8 == e, total, 0.0)
        gate_in[t_me] = value[:experts]
        for i in range(tp - 1):
            gate_tp(i).start()

    def gates_on():
        for i in range(tp - 1):
            q = lax.rem(t_me + 1 + i, tp)
            pltpu.make_async_remote_copy(
                src_ref=gate_in.at[q], dst_ref=gate_in.at[q],
                send_sem=gt_send.at[i], recv_sem=gt_recv.at[q],
                device_id=(e_me, q), device_id_type=MESH).wait_recv()
        total = gate_in[0]
        for q in range(1, tp):
            total = total + gate_in[q]
        for i in range(slots // lanes):
            gate_sum[i] = total[:, i * lanes : (i + 1) * lanes]
        gate_back[e_me] = gate_sum[tile_of(e_me)]
        for d in others:
            gate_ep(d).start()

    def weight_grads(q):
        alone(lambda: weight_quarter(q))

    def weight_quarter(q):
        x_t = rows_in[q, :, pl.ds(0, cs)].T
        yq = rows_in[q, :, pl.ds(cs, cs)]
        for e in range(experts):
            vwg[e, share(q), :] = dot(x_t, gate_b[e]).astype(bf16)
            vwu[e, share(q), :] = dot(x_t, up_b[e]).astype(bf16)
            vwd[e, :, share(q)] = dot(act_c[e], yq, TN).astype(bf16)

    near = others[1:ep // 2 - 1] + others[:1]
    far_b = others[:-1 - ep // 4:-1]
    far_c = others[-1 - ep // 4:ep // 2 - 2:-1]
    far = far_b + far_c
    a, f = chunk_of(0, ep // 2), chunk_of(ep // 2, ep // 2)
    b, c = chunk_of(far_b[0], ep // 4), chunk_of(far_c[0], ep // 4)

    def c_arrived(ds):
        for d in ds:
            e = xor(d)
            pltpu.make_async_remote_copy(
                src_ref=c_out.at[0], dst_ref=c_in.at[e], send_sem=c_send.at[0],
                recv_sem=c_recv.at[e], device_id=(e_me, partner), device_id_type=MESH).wait_recv()

    to_chips(near)
    for load in loads[7:]:
        load.wait()
    wait_own(near)
    first_half(a)
    to_chips(far_b)
    relay(near[::-1])
    wait_last(near)
    c_arrived(near)
    second_half(a)
    to_chips(far_c[:1])
    dx_first(0, a)
    to_chips(far_c[1:])
    relay(far_b)
    dx_rest(0, a)
    wait_own(far)
    first_half(f)
    dx_over(0, a, near + [0])
    wait_last(far_b)
    c_arrived(far)
    second_half(b)
    relay(far_c[:1])
    dx_first(1, b)
    alone(lambda: dx_other_chip(b))
    relay(far_c[1:])
    alone(lambda: dx_my_chip(1, b))
    dx_over(1, b, far_b)
    own_ready(0, a)
    wait_last(far_c)
    second_half(c)
    dx_first(2, c)
    alone(lambda: dx_other_chip(c))
    gates()
    dx_over(2, c, far_c)
    alone(lambda: dx_my_chip(2, c))
    own_ready(1, b)
    send_back(far_b)
    send_back(near + [0])
    weight_grads(0)
    gates_on()
    own_ready(2, c)
    weight_grads(1)
    send_back(far_c)
    weight_grads(2)
    weight_grads(3)

    def returned(d):
        g = xor(d)
        pltpu.make_async_remote_copy(
            src_ref=gate_sum.at[0], dst_ref=gate_back.at[g],
            send_sem=ge_send.at[0], recv_sem=ge_recv.at[g],
            device_id=(g, partner), device_id_type=MESH).wait_recv()

    def rows_back(d):
        g = xor(d)
        pltpu.make_async_remote_copy(
            src_ref=to_ep.at[block(g)], dst_ref=back.at[block(g)],
            send_sem=dxe_send.at[0], recv_sem=dxe_recv.at[g],
            device_id=(g, partner), device_id_type=MESH).wait_recv()

    for d in others:
        returned(d)
    for d in range(ep):
        rows_back(d)
    send_wide().wait_send()
    for d in range(ep):
        dx_x(d).wait_send()
        dx_ep(d).wait_send()
    for d in others:
        send_rows(d).wait_send()
        send_c(d).wait_send()
        if d != 1:
            pass_on(partner, d, send_x, cross).wait_send()
        pass_on(partner, d, send_p, partner).wait_send()
        relayed(d).wait_send()
        gate_ep(d).wait_send()
    for i, chunk in enumerate((a, b, c)):
        for k in range(2):
            dx_partner(k, i, chunk).wait_send()
    for i in range(tp - 1):
        gate_tp(i).wait_send()


def finish(
    place_ref, back, gate_back, vwg, vwu, vwd, gid_ref, wid_ref,
    dtok_ref, dgate_ref, gwg_ref, gwu_ref, gwd_ref, dtok, dgate, sem,
):
    copies = []
    for a, b in ((vwg, gwg_ref), (vwu, gwu_ref), (vwd, gwd_ref)):
        experts, rows, _ = a.shape
        for e in range(experts):
            for half in range(2):
                part = pl.ds(half * (rows // 2), rows // 2)
                copies.append(pltpu.make_async_copy(
                    a.at[e, part], b.at[e, part], sem.at[2 + len(copies)]))
    for copy in copies:
        copy.start()
    ep, per, slots = gate_back.shape
    tok_rows = place_ref.shape[2]
    dtok[...] = dot(place_ref[0], back[...], TN).astype(jnp.bfloat16)
    copies.append(pltpu.make_async_copy(dtok, dtok_ref, sem.at[0]))
    copies[-1].start()
    sums = jnp.concatenate([gate_back[e] for e in range(ep)], axis=0)
    high = sums.astype(jnp.bfloat16)
    low = (sums - high.astype(jnp.float32)).astype(jnp.bfloat16)
    pick = place_ref[1, :slots, :]
    dense = dot(high, pick) + dot(low, pick)
    row = lax.broadcasted_iota(jnp.int32, (ep * per, tok_rows), 0)
    for k in range(wid_ref.shape[0]):
        wanted = row == gid_ref[...] * per + wid_ref[k : k + 1, :]
        dgate[k : k + 1, :] = jnp.sum(jnp.where(wanted, dense, 0.0), axis=0, keepdims=True)
    copies.append(pltpu.make_async_copy(dgate, dgate_ref, sem.at[1]))
    copies[-1].start()
    for copy in copies:
        copy.wait()


def on_device(tokens, cotangent, group_ids, within_ids, gate_weights, w_gate, w_up, w_down):
    ep = lax.axis_size("ep")
    tp = lax.axis_size("tp")
    tok_rows, width = tokens.shape
    experts, _, ff = w_gate.shape
    cap = (3 * tok_rows + 2 * ep - 1) // (2 * ep)
    cap = -(-cap // 16) * 16
    slots = ep * cap
    gate_lanes = LANES if LANES % cap == 0 and slots % LANES == 0 else slots
    cs = width // tp
    nx = tp // 2
    bf16, f32 = jnp.bfloat16, jnp.float32
    dma = pltpu.SemaphoreType.DMA
    hbm = pl.BlockSpec(memory_space=pltpu.HBM)
    vmem = pl.BlockSpec(memory_space=pltpu.VMEM)
    scratch = [
        pltpu.VMEM((tok_rows, 2 * cs), bf16),
        pltpu.VMEM((slots, 2 * cs + LANES), bf16),
        pltpu.VMEM((tp, slots, 2 * cs + LANES), bf16),
        pltpu.VMEM(w_gate.shape, bf16),
        pltpu.VMEM(w_up.shape, bf16),
        pltpu.VMEM(w_down.shape, bf16),
        pltpu.VMEM((experts, 3, slots, ff), f32),
        pltpu.VMEM((experts, slots, ff), bf16),
        pltpu.VMEM((experts, slots, ff), bf16),
        pltpu.VMEM((experts, slots, ff), bf16),
        pltpu.VMEM((nx, slots, cs), bf16),
        pltpu.VMEM((nx, slots, cs), bf16),
        pltpu.VMEM((slots, cs), f32),
        pltpu.VMEM((nx - 1, slots, cs), bf16),
        pltpu.VMEM((nx - 1, slots, cs), bf16),
        pltpu.VMEM((slots, cs), bf16),
        pltpu.VMEM((tp, 8, slots), f32),
        pltpu.VMEM((8, slots), f32),
        dma((5,)), dma((1,)), dma((ep,)), dma((tp, ep)),
        dma((nx - 1, ep)), dma((ep,)), dma((nx - 1, ep)),
        dma((nx,)), dma((nx,)), dma((nx - 1, ep)), dma((nx - 1, ep)), dma((ep,)), dma((ep,)),
        dma((tp,)), dma((tp,)), dma((ep,)), dma((ep,)),
    ]
    gid, wid, gw = group_ids.T, within_ids.T, gate_weights.T
    body, per, small = kernel, 8, vmem
    if ep == 8 and tp == 4 and gate_lanes == LANES:
        body, per, small = fast_kernel, experts, hbm
        scratch = [
            pltpu.VMEM(gid.shape, jnp.int32),
            pltpu.VMEM(wid.shape, jnp.int32),
            pltpu.VMEM(gw.shape, bf16),
            pltpu.VMEM((tok_rows, 2 * cs), bf16),
            pltpu.VMEM((tok_rows, width), bf16),
            pltpu.VMEM((tok_rows, width), bf16),
            pltpu.VMEM((slots, 2 * cs), bf16),
            pltpu.VMEM((tp, slots, 2 * cs), bf16),
            pltpu.VMEM(w_gate.shape, bf16),
            pltpu.VMEM(w_up.shape, bf16),
            pltpu.VMEM(w_down.shape, bf16),
            pltpu.VMEM((cap, 2 * cs), bf16),
            pltpu.VMEM((experts, 3, slots, ff), f32),
            pltpu.VMEM((experts, slots, ff), bf16),
            pltpu.VMEM((experts, slots, ff), bf16),
            pltpu.VMEM((experts, slots, ff), bf16),
            pltpu.VMEM((experts, slots, ff), bf16),
            pltpu.VMEM((experts, slots, ff), bf16),
            pltpu.VMEM((slots // gate_lanes, experts, gate_lanes), f32),
            pltpu.VMEM((ep, experts, gate_lanes), f32),
            pltpu.VMEM((2, slots, cs), bf16),
            pltpu.VMEM((2, slots, cs), bf16),
            pltpu.VMEM((slots, cs), f32),
            pltpu.VMEM((slots, cs), f32),
            pltpu.VMEM((slots, cs), bf16),
            pltpu.VMEM((slots, cs), bf16),
            pltpu.VMEM((slots, cs), bf16),
            pltpu.VMEM((tp, experts, slots), f32),
            pltpu.VMEM((slots // gate_lanes, experts, gate_lanes), f32),
            dma((10,)), dma((1,)), dma((ep,)), dma((tp, ep)), dma((ep,)), dma((ep,)), dma((ep,)),
            dma((ep,)), dma((ep,)), dma((2, 3)), dma((2, 3)), dma((ep,)), dma((ep,)),
            dma((ep,)), dma((ep,)), dma((tp,)), dma((tp,)), dma((ep,)), dma((ep,)),
        ]
    kept = pl.pallas_call(
        functools.partial(body, ep, tp, cap),
        out_shape=(
            pltpu.VMEM((2, slots, tok_rows), bf16),
            pltpu.VMEM((slots, cs), bf16),
            pltpu.VMEM((ep, per, gate_lanes), f32),
            pltpu.VMEM(w_gate.shape, bf16),
            pltpu.VMEM(w_up.shape, bf16),
            pltpu.VMEM(w_down.shape, bf16),
        ),
        in_specs=[hbm, hbm, small, small, small, hbm, hbm, hbm],
        out_specs=(vmem,) * 6,
        scratch_shapes=scratch,
        compiler_params=pltpu.CompilerParams(
            collective_id=0, has_side_effects=True, vmem_limit_bytes=57 * 1024 * 1024),
    )(tokens, cotangent, gid, wid, gw, w_gate, w_up, w_down)
    dtok, dgate, gwg, gwu, gwd = pl.pallas_call(
        finish,
        out_shape=(
            jax.ShapeDtypeStruct((tok_rows, cs), bf16),
            jax.ShapeDtypeStruct(wid.shape, f32),
            jax.ShapeDtypeStruct(w_gate.shape, bf16),
            jax.ShapeDtypeStruct(w_up.shape, bf16),
            jax.ShapeDtypeStruct(w_down.shape, bf16),
        ),
        in_specs=[vmem] * 8,
        out_specs=(hbm,) * 5,
        scratch_shapes=[
            pltpu.VMEM((tok_rows, cs), bf16),
            pltpu.VMEM(wid.shape, f32),
            dma((2 + 6 * experts,)),
        ],
        compiler_params=pltpu.CompilerParams(vmem_limit_bytes=12 * 1024 * 1024),
    )(*kept, gid, wid)
    return dtok, dgate.T, gwg, gwu, gwd


def solution(mesh):
    in_specs = (
        P("ep", None),
        P("ep", None),
        P("ep", None),
        P("ep", None),
        P("ep", None),
        P("ep", None, "tp"),
        P("ep", None, "tp"),
        P("ep", "tp", None),
    )
    out_specs = (
        P("ep", "tp"),
        P("ep", None),
        P("ep", None, "tp"),
        P("ep", None, "tp"),
        P("ep", "tp", None),
    )
    return jax.shard_map(
        on_device, mesh=mesh, in_specs=in_specs, out_specs=out_specs, check_vma=False
    )
```

```python
import functools

import jax
import jax.numpy as jnp
from jax import lax
from jax.experimental import pallas as pl
from jax.experimental.pallas import tpu as pltpu
from jax.sharding import PartitionSpec as P

MESH = pl.DeviceIdType.MESH
LANES = 128
NT = (((1,), (1,)), ((), ()))
TN = (((0,), (0,)), ((), ()))
NN = (((1,), (0,)), ((), ()))


def dot(a, b, dims=NN):
    return lax.dot_general(a, b, dims, preferred_element_type=jnp.float32)


def each(count, body):
    if count <= 8:
        for i in range(count):
            body(i)
    else:
        lax.fori_loop(0, count, lambda i, c: (body(i), c)[1], 0)


def aligned(value, step):
    return value if isinstance(value, int) else pl.multiple_of(value, step)


def kernel(
    ep, tp, cap,
    tok_ref, cot_ref, gid_ref, wid_ref, gw_ref, wg_ref, wu_ref, wd_ref,
    place_ref, back, gate_back, vwg, vwu, vwd,
    src, placed, rows_in, wg, wu, wd, acc, gate_b, up_b, act_c,
    to_partner, from_partner, dx_acc, to_x, from_x, to_ep,
    gate_in, gate_sum,
    load_sem, own_sem, send1, recv_rows, send_x, send_p, send_p2,
    dxp_send, dxp_recv, dxx_send, dxx_recv, dxe_send, dxe_recv,
    gt_send, gt_recv, ge_send, ge_recv,
):
    e_me = lax.axis_index("ep")
    t_me = lax.axis_index("tp")
    core = lax.rem(t_me, 2)
    x_me = lax.div(t_me, 2)
    partner = t_me + 1 - 2 * core
    nx = tp // 2
    gate_lanes = gate_back.shape[2]
    tok_rows, width = tok_ref.shape
    cs = width // tp
    slots = ep * cap
    experts = wg.shape[0]
    bf16 = jnp.bfloat16

    barrier = pltpu.get_barrier_semaphore()
    each(ep - 1, lambda i: pl.semaphore_signal(
        barrier, inc=1, device_id=(lax.rem(e_me + 1 + i, ep), t_me), device_id_type=MESH))
    each(tp - 1, lambda i: pl.semaphore_signal(
        barrier, inc=1, device_id=(e_me, lax.rem(t_me + 1 + i, tp)), device_id_type=MESH))

    my_cols = pl.ds(pl.multiple_of(t_me * cs, LANES), cs)
    loads = [
        pltpu.make_async_copy(tok_ref.at[:, my_cols], src.at[:, pl.ds(0, cs)], load_sem.at[0]),
        pltpu.make_async_copy(cot_ref.at[:, my_cols], src.at[:, pl.ds(cs, cs)], load_sem.at[1]),
        pltpu.make_async_copy(wg_ref, wg, load_sem.at[2]),
        pltpu.make_async_copy(wu_ref, wu, load_sem.at[3]),
        pltpu.make_async_copy(wd_ref, wd, load_sem.at[4]),
    ]
    for load in loads[:2]:
        load.start()

    group = gid_ref[...]
    groups = -(-ep // 16) * 16
    in_group = (
        lax.broadcasted_iota(jnp.int32, (groups, tok_rows), 0) == group
    ).astype(jnp.float32)
    earlier = (
        lax.broadcasted_iota(jnp.int32, (tok_rows, tok_rows), 0)
        < lax.broadcasted_iota(jnp.int32, (tok_rows, tok_rows), 1)
    ).astype(jnp.float32).astype(bf16)
    before = dot(in_group.astype(bf16), earlier)
    rank = jnp.sum(before * in_group, axis=0, keepdims=True).astype(jnp.int32)
    slot_row = lax.broadcasted_iota(jnp.int32, (slots, tok_rows), 0)
    place = (slot_row == group * cap + rank).astype(jnp.float32).astype(bf16)
    place_ref[0] = place
    place_ref[1] = (slot_row == e_me * cap % gate_lanes + rank).astype(jnp.float32).astype(bf16)
    lane_row = lax.broadcasted_iota(jnp.int32, (LANES, tok_rows), 0)
    weights = gw_ref[...].astype(jnp.float32)
    comb = jnp.zeros((LANES, tok_rows), jnp.float32)
    for k in range(weights.shape[0]):
        comb = comb + jnp.where(lane_row == wid_ref[k : k + 1, :], weights[k : k + 1, :], 0.0)
    placed[:, pl.ds(2 * cs, LANES)] = dot(place, comb.astype(bf16), NT).astype(bf16)
    loads[0].wait()
    placed[:, pl.ds(0, cs)] = dot(place, src[:, pl.ds(0, cs)]).astype(bf16)
    loads[1].wait()
    for load in loads[2:]:
        load.start()
    placed[:, pl.ds(cs, cs)] = dot(place, src[:, pl.ds(cs, cs)]).astype(bf16)

    pl.semaphore_wait(barrier, ep + tp - 2)

    def xor(d):
        value, bit = 0, 1
        while bit < ep:
            value = value + (e_me // bit + d // bit) % 2 * bit
            bit *= 2
        return value

    def target(d):
        return xor(d) if ep & (ep - 1) == 0 else lax.rem(e_me + d, ep)

    def source(d):
        return xor(d) if ep & (ep - 1) == 0 else lax.rem(e_me - d + ep, ep)

    def block(e):
        return pl.ds(aligned(e * cap, 16), cap)

    distances = list(range(ep))
    def stage1(d):
        g = target(d)
        return pltpu.make_async_remote_copy(
            src_ref=placed.at[block(g)], dst_ref=rows_in.at[t_me, block(e_me)],
            send_sem=send1.at[d], recv_sem=recv_rows.at[t_me, e_me],
            device_id=(g, t_me), device_id_type=MESH)

    own = pltpu.make_async_copy(
        placed.at[block(e_me)], rows_in.at[t_me, block(e_me)], own_sem.at[0])
    own.start()
    if ep <= 8:
        for d in distances[1:]:
            stage1(d).start()
    else:
        each(ep - 1, lambda i: stage1(i + 1).start())

    def arrived(q, e, cols):
        part = rows_in.at[q, block(e), pl.ds(0, cols)]
        pltpu.make_async_remote_copy(
            src_ref=part, dst_ref=part, send_sem=send1.at[0], recv_sem=recv_rows.at[q, e],
            device_id=(e_me, partner), device_id_type=MESH).wait_recv()

    def forward(q, e, sem, target):
        part = rows_in.at[q, block(e), pl.ds(0, 2 * cs)]
        return pltpu.make_async_remote_copy(
            src_ref=part, dst_ref=part, send_sem=sem, recv_sem=recv_rows.at[q, e],
            device_id=(e_me, target), device_id_type=MESH)

    def x_peer(k):
        return lax.rem(x_me + k, nx) * 2 + core

    def to_peers(d):
        e = source(d)
        copies = [forward(t_me, e, send_x.at[k - 1, d], x_peer(k)) for k in range(1, nx)]
        return copies + [forward(t_me, e, send_p.at[d], partner)]

    def stage2(d):
        for copy in to_peers(d):
            copy.start()

    def relays(d):
        e = source(d)
        return [(x_peer(k), e, forward(x_peer(k), e, send_p2.at[k - 1, d], partner))
                for k in range(1, nx)]

    def stage3(d):
        for q, e, copy in relays(d):
            arrived(q, e, 2 * cs)
            copy.start()

    own.wait()
    stage2(0)
    if ep <= 8:
        for i, d in enumerate(distances[1:]):
            arrived(t_me, source(d), 2 * cs + LANES)
            stage2(d)
    else:
        def later(i):
            arrived(t_me, source(i + 1), 2 * cs + LANES)
            stage2(i + 1)
        each(ep - 1, later)

    for load in loads[2:]:
        load.wait()

    def share(q):
        return pl.ds(aligned(q * cs, LANES), cs)

    def hidden(q, first):
        xq = rows_in[q, :, pl.ds(0, cs)]
        yq = rows_in[q, :, pl.ds(cs, cs)]
        for e in range(experts):
            for n, value in enumerate((
                dot(xq, wg[e, share(q), :]),
                dot(xq, wu[e, share(q), :]),
                dot(yq, wd[e, :, share(q)], NT),
            )):
                acc[e, n] = value if first else acc[e, n] + value

    def all_arrived(q):
        each(ep, lambda e: arrived(q, e, 2 * cs))

    hidden(t_me, True)
    if ep <= 8:
        for d in distances:
            stage3(d)
    else:
        each(ep, stage3)
    all_arrived(partner)
    hidden(partner, False)

    def x_quarters(k):
        hidden(x_peer(k), False)
        other = lax.rem(x_me + k, nx) * 2 + 1 - core
        all_arrived(other)
        hidden(other, False)
    each(nx - 1, lambda i: x_quarters(i + 1))

    row8 = lax.broadcasted_iota(jnp.int32, (8, slots), 0)
    gates = jnp.zeros((8, slots), jnp.float32)
    for e in range(experts):
        pre_gate, pre_up, dy_down = acc[e, 0], acc[e, 1], acc[e, 2]
        c = rows_in[t_me, :, pl.ds(2 * cs, LANES)][:, e : e + 1].astype(jnp.float32)
        sig = jax.nn.sigmoid(pre_gate)
        silu = pre_gate * sig
        act = silu * pre_up
        prod = act.astype(bf16).astype(jnp.float32) * dy_down
        act_grad = c * dy_down
        act_c[e] = (c * act).astype(bf16)
        gate_b[e] = (act_grad * pre_up * sig * (1.0 + pre_gate * (1.0 - sig))).astype(bf16)
        up_b[e] = (act_grad * silu).astype(bf16)
        high = prod.astype(bf16)
        low = (prod - high.astype(jnp.float32)).astype(bf16)
        ones = jnp.ones((8, prod.shape[1]), bf16)
        gates = gates + jnp.where(row8 == e, dot(ones, high, NT) + dot(ones, low, NT), 0.0)
    gate_in[t_me] = gates

    def gate_tp(i):
        return pltpu.make_async_remote_copy(
            src_ref=gate_in.at[t_me], dst_ref=gate_in.at[t_me],
            send_sem=gt_send.at[i], recv_sem=gt_recv.at[t_me],
            device_id=(e_me, lax.rem(t_me + 1 + i, tp)), device_id_type=MESH)

    def dx_of(q):
        total = None
        for e in range(experts):
            part = dot(gate_b[e], wg[e, share(q), :], NT) + dot(up_b[e], wu[e, share(q), :], NT)
            total = part if total is None else total + part
        return total

    def dx_partner(k):
        return pltpu.make_async_remote_copy(
            src_ref=to_partner.at[k], dst_ref=from_partner.at[k],
            send_sem=dxp_send.at[k], recv_sem=dxp_recv.at[k],
            device_id=(e_me, partner), device_id_type=MESH)

    def give_partner(i):
        k = nx - 1 - i
        to_partner[k] = dx_of(lax.rem(x_me + k, nx) * 2 + 1 - core).astype(bf16)
        dx_partner(k).start()

    def dx_x(k, d):
        e = target(d)
        return pltpu.make_async_remote_copy(
            src_ref=to_x.at[k - 1, block(e)], dst_ref=from_x.at[k - 1, block(e)],
            send_sem=dxx_send.at[k - 1, d], recv_sem=dxx_recv.at[k - 1, d],
            device_id=(e_me, x_peer(k)), device_id_type=MESH)

    far = distances[::-1]

    def walk(body):
        if ep <= 8:
            for i, d in enumerate(far):
                body(i, d)
        else:
            each(ep, lambda i: body(i, ep - 1 - i))

    def give_x(k):
        mine = dx_of(x_peer(k))
        dx_partner(k).wait_recv()
        to_x[k - 1] = (mine + from_partner[k].astype(jnp.float32)).astype(bf16)
        walk(lambda i, d: dx_x(k, d).start())
    each(tp - 1, lambda i: gate_tp(i).start())

    def cross(i):
        give_partner(i)
        give_x(nx - 1 - i)
    each(nx - 1, cross)
    give_partner(nx - 1)
    mine = dx_of(t_me)
    dx_partner(0).wait_recv()
    dx_acc[...] = mine + from_partner[0].astype(jnp.float32)

    def gate_tile(e):
        return pl.ds(pl.multiple_of(e * cap // gate_lanes * gate_lanes, LANES), gate_lanes)

    def gate_ep(d):
        return pltpu.make_async_remote_copy(
            src_ref=gate_sum.at[:, gate_tile(target(d))], dst_ref=gate_back.at[e_me],
            send_sem=ge_send.at[d], recv_sem=ge_recv.at[e_me],
            device_id=(target(d), t_me), device_id_type=MESH)

    def gate_wait(i):
        q = lax.rem(t_me + 1 + i, tp)
        pltpu.make_async_remote_copy(
            src_ref=gate_in.at[q], dst_ref=gate_in.at[q],
            send_sem=gt_send.at[i], recv_sem=gt_recv.at[q],
            device_id=(e_me, q), device_id_type=MESH).wait_recv()

    def gates_on():
        each(tp - 1, gate_wait)
        total = gate_in[0]
        for q in range(1, tp):
            total = total + gate_in[q]
        gate_sum[...] = total
        gate_back[e_me] = gate_sum[:, gate_tile(e_me)]
        each(ep - 1, lambda i: gate_ep(i + 1).start())

    def weight_grads(q):
        x_t = rows_in[q, :, pl.ds(0, cs)].T
        yq = rows_in[q, :, pl.ds(cs, cs)]
        for e in range(experts):
            vwg[e, share(q), :] = dot(x_t, gate_b[e]).astype(bf16)
            vwu[e, share(q), :] = dot(x_t, up_b[e]).astype(bf16)
            vwd[e, :, share(q)] = dot(act_c[e], yq, TN).astype(bf16)

    def dx_ep(d):
        g = target(d)
        return pltpu.make_async_remote_copy(
            src_ref=to_ep.at[block(g)], dst_ref=back.at[block(e_me)],
            send_sem=dxe_send.at[d], recv_sem=dxe_recv.at[e_me],
            device_id=(g, t_me), device_id_type=MESH)

    def finish_chunk(d):
        rows = block(target(d))
        value = dx_acc[rows, :]
        for k in range(1, nx):
            dx_x(k, d).wait_recv()
            value = value + from_x[k - 1, rows, :].astype(jnp.float32)
        return value.astype(bf16)

    def chunk(i, d):
        to_ep[block(target(d)), :] = finish_chunk(d)
        dx_ep(d).start()

    if ep <= 8:
        done = 0
        for i, d in enumerate(far[:-1]):
            chunk(i, d)
            if i % 2 == 0 and done < tp:
                weight_grads(done)
                done += 1
            if i == min(2, ep - 2):
                gates_on()
        for q in range(done, tp):
            weight_grads(q)
    else:
        each(ep - 1, lambda i: chunk(i, ep - 1 - i))
        each(tp, weight_grads)
        gates_on()
    back[block(e_me), :] = finish_chunk(0)

    def gate_arrived(i):
        g = lax.rem(e_me + 1 + i, ep)
        pltpu.make_async_remote_copy(
            src_ref=gate_sum.at[:, gate_tile(g)], dst_ref=gate_back.at[g],
            send_sem=ge_send.at[0], recv_sem=ge_recv.at[g],
            device_id=(g, t_me), device_id_type=MESH).wait_recv()
    each(ep - 1, gate_arrived)
    def back_arrived(i):
        g = lax.rem(e_me + 1 + i, ep)
        pltpu.make_async_remote_copy(
            src_ref=to_ep.at[block(g)], dst_ref=back.at[block(g)],
            send_sem=dxe_send.at[0], recv_sem=dxe_recv.at[g],
            device_id=(g, t_me), device_id_type=MESH).wait_recv()
    each(ep - 1, back_arrived)

    def sent1(i):
        d = i + 1
        stage1(d).wait_send()
        gate_ep(d).wait_send()
        dx_ep(d).wait_send()
    each(ep - 1, sent1)

    def sent2(d):
        for copy in to_peers(d):
            copy.wait_send()
        for _, _, copy in relays(d):
            copy.wait_send()
        for k in range(1, nx):
            dx_x(k, d).wait_send()
    each(ep, sent2)
    each(nx, lambda k: dx_partner(k).wait_send())
    each(tp - 1, lambda i: gate_tp(i).wait_send())


def fast_kernel(
    ep, tp, cap,
    tok_ref, cot_ref, gid_ref, wid_ref, gw_ref, wg_ref, wu_ref, wd_ref,
    place_ref, back, gate_back, vwg, vwu, vwd,
    gid, wid, gw, src, tok_all, cot_all, placed, rows_in, wg, wu, wd,
    wide, acc, gate_b, up_b, act_c, prod_hi, prod_lo, c_out, c_in,
    to_partner, from_partner, dx_acc, dx_far, to_x, from_x, to_ep, gate_in, gate_sum,
    load_sem, wide_send, send1, recv_rows, send_p, send_x, send_r, c_send, c_recv,
    dxp_send, dxp_recv, dxx_send, dxx_recv, dxe_send, dxe_recv,
    gt_send, gt_recv, ge_send, ge_recv,
):
    e_me = lax.axis_index("ep")
    t_me = lax.axis_index("tp")
    core = lax.rem(t_me, 2)
    x_me = lax.div(t_me, 2)
    x_other = 1 - x_me
    partner = 2 * x_me + 1 - core
    cross = 2 * x_other + 1 - core
    beyond = 2 * x_other + core
    lanes = gate_back.shape[2]
    tok_rows, width = tok_ref.shape
    cs = width // tp
    slots = ep * cap
    experts = wg.shape[0]
    bf16 = jnp.bfloat16

    barrier = pltpu.get_barrier_semaphore()
    for i in range(ep - 1):
        pl.semaphore_signal(
            barrier, inc=1, device_id=(lax.rem(e_me + 1 + i, ep), partner), device_id_type=MESH)
    for i in range(tp - 1):
        pl.semaphore_signal(
            barrier, inc=1, device_id=(e_me, lax.rem(t_me + 1 + i, tp)), device_id_type=MESH)

    my_cols = pl.ds(pl.multiple_of(t_me * cs, LANES), cs)
    loads = [pltpu.make_async_copy(a, b, load_sem.at[i]) for i, (a, b) in enumerate((
        (gid_ref, gid), (wid_ref, wid), (gw_ref, gw),
        (tok_ref.at[:, my_cols], src.at[:, pl.ds(0, cs)]),
        (cot_ref.at[:, my_cols], src.at[:, pl.ds(cs, cs)]),
        (tok_ref, tok_all), (cot_ref, cot_all),
        (wg_ref, wg), (wu_ref, wu), (wd_ref, wd),
    ))]
    for load in loads[:5]:
        load.start()
    earlier = (
        lax.broadcasted_iota(jnp.int32, (tok_rows, tok_rows), 0)
        < lax.broadcasted_iota(jnp.int32, (tok_rows, tok_rows), 1)
    ).astype(jnp.float32).astype(bf16)
    slot_row = lax.broadcasted_iota(jnp.int32, (slots, tok_rows), 0)
    for load in loads[:3]:
        load.wait()

    group = gid[...]
    groups = -(-ep // 16) * 16
    in_group = (
        lax.broadcasted_iota(jnp.int32, (groups, tok_rows), 0) == group
    ).astype(jnp.float32)
    before = dot(in_group.astype(bf16), earlier)
    rank = jnp.sum(before * in_group, axis=0, keepdims=True).astype(jnp.int32)
    place = (slot_row == group * cap + rank).astype(jnp.float32).astype(bf16)
    place_ref[0] = place
    loads[3].wait()
    placed[:, pl.ds(0, cs)] = dot(place, src[:, pl.ds(0, cs)]).astype(bf16)
    loads[4].wait()
    placed[:, pl.ds(cs, cs)] = dot(place, src[:, pl.ds(cs, cs)]).astype(bf16)
    for load in loads[5:]:
        load.start()

    def xor(d):
        value, bit = 0, 1
        while bit < ep:
            value = value + (e_me // bit + d // bit) % 2 * bit
            bit *= 2
        return value

    def block(e):
        return pl.ds(aligned(e * cap, 16), cap)

    def tile_of(e):
        return e * cap // lanes

    pl.semaphore_wait(barrier, ep + tp - 2)

    def send_rows(d):
        g = xor(d)
        return pltpu.make_async_remote_copy(
            src_ref=placed.at[block(g)], dst_ref=rows_in.at[t_me, block(e_me)],
            send_sem=send1.at[d], recv_sem=recv_rows.at[t_me, e_me],
            device_id=(g, partner), device_id_type=MESH)

    def send_c(d):
        g = xor(d)
        return pltpu.make_async_remote_copy(
            src_ref=c_out.at[tile_of(g)], dst_ref=c_in.at[e_me],
            send_sem=c_send.at[d], recv_sem=c_recv.at[e_me],
            device_id=(g, partner), device_id_type=MESH)

    others = list(range(1, ep))
    def send_wide():
        return pltpu.make_async_remote_copy(
            src_ref=wide, dst_ref=rows_in.at[beyond, block(e_me)],
            send_sem=wide_send.at[0], recv_sem=recv_rows.at[beyond, e_me],
            device_id=(xor(1), partner), device_id_type=MESH)

    for d in others[1:ep // 2 - 1] + others[:1]:
        send_rows(d).start()
    lane_row = lax.broadcasted_iota(jnp.int32, (16, tok_rows), 0)
    weights = gw[...].astype(jnp.float32)
    comb = jnp.zeros((16, tok_rows), jnp.float32)
    for k in range(weights.shape[0]):
        comb = comb + jnp.where(lane_row == wid[k : k + 1, :], weights[k : k + 1, :], 0.0)
    c_rows = dot(comb.astype(bf16), place, NT)
    for i in range(slots // lanes):
        c_out[i] = c_rows[:experts, i * lanes : (i + 1) * lanes]
    for d in others[:ep // 2 - 1]:
        send_c(d).start()
    for d in others[:ep // 2 - 2:-1]:
        send_rows(d).start()
    for d in others[ep // 2 - 1:]:
        send_c(d).start()
    loads[5].wait()
    loads[6].wait()
    beside = place_ref[0, block(xor(1)), :]
    far_cols = pl.ds(pl.multiple_of(beyond * cs, LANES), cs)
    wide[:, pl.ds(0, cs)] = dot(beside, tok_all[:, far_cols]).astype(bf16)
    wide[:, pl.ds(cs, cs)] = dot(beside, cot_all[:, far_cols]).astype(bf16)
    send_wide().start()

    def arrived(q, d):
        e = xor(d)
        part = rows_in.at[q, block(e)]
        pltpu.make_async_remote_copy(
            src_ref=part, dst_ref=part, send_sem=send1.at[0], recv_sem=recv_rows.at[q, e],
            device_id=(e_me, partner), device_id_type=MESH).wait_recv()

    def pass_on(q, d, sem, device):
        e = xor(d)
        part = rows_in.at[q, block(e)]
        return pltpu.make_async_remote_copy(
            src_ref=part, dst_ref=part, send_sem=sem.at[d], recv_sem=recv_rows.at[q, e],
            device_id=(e_me, device), device_id_type=MESH)

    def to_chips(ds):
        for d in ds:
            arrived(partner, d)
            if d != 1:
                pass_on(partner, d, send_x, cross).start()
            pass_on(partner, d, send_p, partner).start()

    def relayed(d):
        return pass_on(cross if d == 1 else beyond, d, send_r, partner)

    def relay(ds):
        for d in ds:
            arrived(cross if d == 1 else beyond, d)
            relayed(d).start()

    def wait_own(ds):
        for d in ds:
            arrived(t_me, d)

    def wait_last(ds):
        for d in ds:
            arrived(beyond if d == 1 else cross, d)

    own = place_ref[0, block(e_me), :]
    own_x = dot(own, tok_all[...]).astype(bf16)
    own_y = dot(own, cot_all[...]).astype(bf16)
    for q in range(tp):
        rows_in[q, block(e_me), pl.ds(0, cs)] = own_x[:, q * cs : (q + 1) * cs]
        rows_in[q, block(e_me), pl.ds(cs, cs)] = own_y[:, q * cs : (q + 1) * cs]
    c_in[e_me] = c_out[tile_of(e_me)]
    place_ref[1] = (slot_row == e_me * cap % lanes + rank).astype(jnp.float32).astype(bf16)

    def chunk_of(d, n):
        first = xor(d)
        first = first - lax.rem(first, n)
        return first, n, pl.ds(pl.multiple_of(first * cap, cap), n * cap)

    def share(q):
        return pl.ds(aligned(q * cs, LANES), cs)

    def lhs(x, rows, first):
        return jnp.concatenate(
            [rows_in[2 * x + i, rows, pl.ds(first, cs)] for i in range(2)], axis=1)

    def half(chunk, x, keep):
        rows = chunk[2]
        xs, ys = lhs(x, rows, 0), lhs(x, rows, cs)
        cols = pl.ds(pl.multiple_of(x * 2 * cs, LANES), 2 * cs)
        out = []
        for e in range(experts):
            values = (dot(xs, wg[e, cols, :]), dot(xs, wu[e, cols, :]), dot(ys, wd[e, :, cols], NT))
            if keep:
                for n, value in enumerate(values):
                    acc[e, n, rows, :] = value
            out.append(values)
        return out

    alone = pl.when(e_me >= 0)

    def keep_half(chunk):
        half(chunk, x_me, True)

    def first_half(chunk):
        alone(lambda: keep_half(chunk))

    lane = lax.broadcasted_iota(jnp.int32, (cap, lanes), 1)
    lane = lane - lax.broadcasted_iota(jnp.int32, (cap, lanes), 0)
    my_lane = lane == lax.rem(e_me * cap, lanes)

    def second_half(chunk):
        alone(lambda: activations(chunk))

    def activations(chunk):
        first, n, rows = chunk
        sums = half(chunk, x_other, False)
        for e in range(experts):
            pre_gate, pre_up, dy_down = (acc[e, m, rows, :] + sums[e][m] for m in range(3))
            c = jnp.concatenate([
                jnp.sum(jnp.where(my_lane, c_in[first + i, e : e + 1, :], 0.0), axis=1, keepdims=True)
                for i in range(n)], axis=0)
            sig = jax.nn.sigmoid(pre_gate)
            silu = pre_gate * sig
            act = silu * pre_up
            prod = act.astype(bf16).astype(jnp.float32) * dy_down
            act_grad = c * dy_down
            act_c[e, rows, :] = (c * act).astype(bf16)
            gate_b[e, rows, :] = (act_grad * pre_up * sig * (1.0 + pre_gate * (1.0 - sig))).astype(bf16)
            up_b[e, rows, :] = (act_grad * silu).astype(bf16)
            high = prod.astype(bf16)
            prod_hi[e, rows, :] = high
            prod_lo[e, rows, :] = (prod - high.astype(jnp.float32)).astype(bf16)

    def dx_of(chunk, q, n):
        rows, total = chunk[2], None
        cols = pl.ds(pl.multiple_of(q * cs, LANES), n * cs)
        for e in range(experts):
            part = dot(gate_b[e, rows, :], wg[e, cols, :], NT)
            part = part + dot(up_b[e, rows, :], wu[e, cols, :], NT)
            total = part if total is None else total + part
        return total

    def dx_partner(k, i, chunk):
        return pltpu.make_async_remote_copy(
            src_ref=to_partner.at[k, chunk[2]], dst_ref=from_partner.at[k, chunk[2]],
            send_sem=dxp_send.at[k, i], recv_sem=dxp_recv.at[k, i],
            device_id=(e_me, partner), device_id_type=MESH)

    def dx_x(d):
        e = xor(d)
        return pltpu.make_async_remote_copy(
            src_ref=to_x.at[block(e)], dst_ref=from_x.at[block(e)],
            send_sem=dxx_send.at[d], recv_sem=dxx_recv.at[d],
            device_id=(e_me, cross), device_id_type=MESH)

    def dx_first(i, chunk):
        @alone
        def _():
            to_partner[0, chunk[2], :] = dx_of(chunk, cross, 1).astype(bf16)
            dx_partner(0, i, chunk).start()

    def dx_rest(i, chunk):
        @alone
        def _():
            dx_other_chip(chunk)
            dx_my_chip(i, chunk)

    def dx_other_chip(chunk):
        dx_far[chunk[2], :] = dx_of(chunk, beyond, 1)

    def dx_my_chip(i, chunk):
        rows = chunk[2]
        both = dx_of(chunk, 2 * x_me, 2)
        low, high = both[:, :cs], both[:, cs:]
        to_partner[1, rows, :] = jnp.where(core == 0, low, high).astype(bf16)
        dx_partner(1, i, chunk).start()
        dx_acc[rows, :] = jnp.where(core == 0, high, low)

    def dx_over(i, chunk, ds):
        dx_partner(0, i, chunk).wait_recv()
        dx_send(ds)

    def dx_send(ds):
        for d in ds:
            rows = block(xor(d))
            to_x[rows, :] = (dx_far[rows, :] + from_partner[0, rows, :].astype(jnp.float32)).astype(bf16)
            dx_x(d).start()

    def dx_ep(d):
        g = xor(d)
        return pltpu.make_async_remote_copy(
            src_ref=to_ep.at[block(g)], dst_ref=back.at[block(e_me)],
            send_sem=dxe_send.at[d], recv_sem=dxe_recv.at[e_me],
            device_id=(g, partner), device_id_type=MESH)

    def own_ready(i, chunk):
        dx_partner(1, i, chunk).wait_recv()

    def send_back(ds):
        for d in ds:
            rows = block(xor(d))
            dx_x(d).wait_recv()
            value = dx_acc[rows, :] + from_partner[1, rows, :].astype(jnp.float32)
            to_ep[rows, :] = (value + from_x[rows, :].astype(jnp.float32)).astype(bf16)
            dx_ep(d).start()

    def gate_tp(i):
        return pltpu.make_async_remote_copy(
            src_ref=gate_in.at[t_me], dst_ref=gate_in.at[t_me],
            send_sem=gt_send.at[i], recv_sem=gt_recv.at[t_me],
            device_id=(e_me, lax.rem(t_me + 1 + i, tp)), device_id_type=MESH)

    def gate_ep(d):
        g = xor(d)
        return pltpu.make_async_remote_copy(
            src_ref=gate_sum.at[tile_of(g)], dst_ref=gate_back.at[e_me],
            send_sem=ge_send.at[d], recv_sem=ge_recv.at[e_me],
            device_id=(g, partner), device_id_type=MESH)

    def gates():
        alone(gate_sums)

    def gate_sums():
        row8 = lax.broadcasted_iota(jnp.int32, (8, slots), 0)
        ones = jnp.ones((8, prod_hi.shape[2]), bf16)
        value = jnp.zeros((8, slots), jnp.float32)
        for e in range(experts):
            total = dot(ones, prod_hi[e], NT) + dot(ones, prod_lo[e], NT)
            value = value + jnp.where(row8 == e, total, 0.0)
        gate_in[t_me] = value[:experts]
        for i in range(tp - 1):
            gate_tp(i).start()

    def gates_on():
        for i in range(tp - 1):
            q = lax.rem(t_me + 1 + i, tp)
            pltpu.make_async_remote_copy(
                src_ref=gate_in.at[q], dst_ref=gate_in.at[q],
                send_sem=gt_send.at[i], recv_sem=gt_recv.at[q],
                device_id=(e_me, q), device_id_type=MESH).wait_recv()
        total = gate_in[0]
        for q in range(1, tp):
            total = total + gate_in[q]
        for i in range(slots // lanes):
            gate_sum[i] = total[:, i * lanes : (i + 1) * lanes]
        gate_back[e_me] = gate_sum[tile_of(e_me)]
        for d in others:
            gate_ep(d).start()

    def weight_grads(q):
        alone(lambda: weight_quarter(q))

    def weight_quarter(q):
        x_t = rows_in[q, :, pl.ds(0, cs)].T
        yq = rows_in[q, :, pl.ds(cs, cs)]
        for e in range(experts):
            vwg[e, share(q), :] = dot(x_t, gate_b[e]).astype(bf16)
            vwu[e, share(q), :] = dot(x_t, up_b[e]).astype(bf16)
            vwd[e, :, share(q)] = dot(act_c[e], yq, TN).astype(bf16)

    near = others[1:ep // 2 - 1] + others[:1]
    far_b = others[:-1 - ep // 4:-1]
    far_c = others[-1 - ep // 4:ep // 2 - 2:-1]
    far = far_b + far_c
    a, f = chunk_of(0, ep // 2), chunk_of(ep // 2, ep // 2)
    b, c = chunk_of(far_b[0], ep // 4), chunk_of(far_c[0], ep // 4)

    def c_arrived(ds):
        for d in ds:
            e = xor(d)
            pltpu.make_async_remote_copy(
                src_ref=c_out.at[0], dst_ref=c_in.at[e], send_sem=c_send.at[0],
                recv_sem=c_recv.at[e], device_id=(e_me, partner), device_id_type=MESH).wait_recv()

    to_chips(near)
    for load in loads[7:]:
        load.wait()
    wait_own(near)
    first_half(a)
    to_chips(far_b)
    relay(near[::-1])
    wait_last(near)
    c_arrived(near)
    second_half(a)
    to_chips(far_c[:1])
    dx_first(0, a)
    to_chips(far_c[1:])
    relay(far_b)
    dx_rest(0, a)
    wait_own(far)
    first_half(f)
    dx_partner(0, 0, a).wait_recv()
    dx_send(near[:-1])
    wait_last(far_b)
    c_arrived(far)
    second_half(b)
    relay(far_c[:1])
    dx_first(1, b)
    alone(lambda: dx_other_chip(b))
    relay(far_c[1:])
    alone(lambda: dx_my_chip(1, b))
    dx_over(1, b, far_b)
    own_ready(0, a)
    wait_last(far_c)
    second_half(c)
    dx_first(2, c)
    alone(lambda: dx_other_chip(c))
    gates()
    dx_over(2, c, far_c)
    dx_send(near[-1:] + [0])
    own_ready(1, b)
    send_back(far_b)
    alone(lambda: dx_my_chip(2, c))
    send_back(near[:-1])
    weight_grads(0)
    gates_on()
    own_ready(2, c)
    weight_grads(1)
    send_back(far_c)
    send_back(near[-1:] + [0])
    weight_grads(2)
    weight_grads(3)

    def returned(d):
        g = xor(d)
        pltpu.make_async_remote_copy(
            src_ref=gate_sum.at[0], dst_ref=gate_back.at[g],
            send_sem=ge_send.at[0], recv_sem=ge_recv.at[g],
            device_id=(g, partner), device_id_type=MESH).wait_recv()

    def rows_back(d):
        g = xor(d)
        pltpu.make_async_remote_copy(
            src_ref=to_ep.at[block(g)], dst_ref=back.at[block(g)],
            send_sem=dxe_send.at[0], recv_sem=dxe_recv.at[g],
            device_id=(g, partner), device_id_type=MESH).wait_recv()

    for d in others:
        returned(d)
    for d in range(ep):
        rows_back(d)
    send_wide().wait_send()
    for d in range(ep):
        dx_x(d).wait_send()
        dx_ep(d).wait_send()
    for d in others:
        send_rows(d).wait_send()
        send_c(d).wait_send()
        if d != 1:
            pass_on(partner, d, send_x, cross).wait_send()
        pass_on(partner, d, send_p, partner).wait_send()
        relayed(d).wait_send()
        gate_ep(d).wait_send()
    for i, chunk in enumerate((a, b, c)):
        for k in range(2):
            dx_partner(k, i, chunk).wait_send()
    for i in range(tp - 1):
        gate_tp(i).wait_send()


def finish(
    place_ref, back, gate_back, vwg, vwu, vwd, gid_ref, wid_ref,
    dtok_ref, dgate_ref, gwg_ref, gwu_ref, gwd_ref, dtok, dgate, sem,
):
    copies = []
    for a, b in ((vwg, gwg_ref), (vwu, gwu_ref), (vwd, gwd_ref)):
        experts, rows, _ = a.shape
        for e in range(experts):
            for half in range(2):
                part = pl.ds(half * (rows // 2), rows // 2)
                copies.append(pltpu.make_async_copy(
                    a.at[e, part], b.at[e, part], sem.at[2 + len(copies)]))
    for copy in copies:
        copy.start()
    ep, per, slots = gate_back.shape
    tok_rows = place_ref.shape[2]
    dtok[...] = dot(place_ref[0], back[...], TN).astype(jnp.bfloat16)
    copies.append(pltpu.make_async_copy(dtok, dtok_ref, sem.at[0]))
    copies[-1].start()
    sums = jnp.concatenate([gate_back[e] for e in range(ep)], axis=0)
    high = sums.astype(jnp.bfloat16)
    low = (sums - high.astype(jnp.float32)).astype(jnp.bfloat16)
    pick = place_ref[1, :slots, :]
    dense = dot(high, pick) + dot(low, pick)
    row = lax.broadcasted_iota(jnp.int32, (ep * per, tok_rows), 0)
    for k in range(wid_ref.shape[0]):
        wanted = row == gid_ref[...] * per + wid_ref[k : k + 1, :]
        dgate[k : k + 1, :] = jnp.sum(jnp.where(wanted, dense, 0.0), axis=0, keepdims=True)
    copies.append(pltpu.make_async_copy(dgate, dgate_ref, sem.at[1]))
    copies[-1].start()
    for copy in copies:
        copy.wait()


def on_device(tokens, cotangent, group_ids, within_ids, gate_weights, w_gate, w_up, w_down):
    ep = lax.axis_size("ep")
    tp = lax.axis_size("tp")
    tok_rows, width = tokens.shape
    experts, _, ff = w_gate.shape
    cap = (3 * tok_rows + 2 * ep - 1) // (2 * ep)
    cap = -(-cap // 16) * 16
    slots = ep * cap
    gate_lanes = LANES if LANES % cap == 0 and slots % LANES == 0 else slots
    cs = width // tp
    nx = tp // 2
    bf16, f32 = jnp.bfloat16, jnp.float32
    dma = pltpu.SemaphoreType.DMA
    hbm = pl.BlockSpec(memory_space=pltpu.HBM)
    vmem = pl.BlockSpec(memory_space=pltpu.VMEM)
    scratch = [
        pltpu.VMEM((tok_rows, 2 * cs), bf16),
        pltpu.VMEM((slots, 2 * cs + LANES), bf16),
        pltpu.VMEM((tp, slots, 2 * cs + LANES), bf16),
        pltpu.VMEM(w_gate.shape, bf16),
        pltpu.VMEM(w_up.shape, bf16),
        pltpu.VMEM(w_down.shape, bf16),
        pltpu.VMEM((experts, 3, slots, ff), f32),
        pltpu.VMEM((experts, slots, ff), bf16),
        pltpu.VMEM((experts, slots, ff), bf16),
        pltpu.VMEM((experts, slots, ff), bf16),
        pltpu.VMEM((nx, slots, cs), bf16),
        pltpu.VMEM((nx, slots, cs), bf16),
        pltpu.VMEM((slots, cs), f32),
        pltpu.VMEM((nx - 1, slots, cs), bf16),
        pltpu.VMEM((nx - 1, slots, cs), bf16),
        pltpu.VMEM((slots, cs), bf16),
        pltpu.VMEM((tp, 8, slots), f32),
        pltpu.VMEM((8, slots), f32),
        dma((5,)), dma((1,)), dma((ep,)), dma((tp, ep)),
        dma((nx - 1, ep)), dma((ep,)), dma((nx - 1, ep)),
        dma((nx,)), dma((nx,)), dma((nx - 1, ep)), dma((nx - 1, ep)), dma((ep,)), dma((ep,)),
        dma((tp,)), dma((tp,)), dma((ep,)), dma((ep,)),
    ]
    gid, wid, gw = group_ids.T, within_ids.T, gate_weights.T
    body, per, small = kernel, 8, vmem
    if ep == 8 and tp == 4 and gate_lanes == LANES:
        body, per, small = fast_kernel, experts, hbm
        scratch = [
            pltpu.VMEM(gid.shape, jnp.int32),
            pltpu.VMEM(wid.shape, jnp.int32),
            pltpu.VMEM(gw.shape, bf16),
            pltpu.VMEM((tok_rows, 2 * cs), bf16),
            pltpu.VMEM((tok_rows, width), bf16),
            pltpu.VMEM((tok_rows, width), bf16),
            pltpu.VMEM((slots, 2 * cs), bf16),
            pltpu.VMEM((tp, slots, 2 * cs), bf16),
            pltpu.VMEM(w_gate.shape, bf16),
            pltpu.VMEM(w_up.shape, bf16),
            pltpu.VMEM(w_down.shape, bf16),
            pltpu.VMEM((cap, 2 * cs), bf16),
            pltpu.VMEM((experts, 3, slots, ff), f32),
            pltpu.VMEM((experts, slots, ff), bf16),
            pltpu.VMEM((experts, slots, ff), bf16),
            pltpu.VMEM((experts, slots, ff), bf16),
            pltpu.VMEM((experts, slots, ff), bf16),
            pltpu.VMEM((experts, slots, ff), bf16),
            pltpu.VMEM((slots // gate_lanes, experts, gate_lanes), f32),
            pltpu.VMEM((ep, experts, gate_lanes), f32),
            pltpu.VMEM((2, slots, cs), bf16),
            pltpu.VMEM((2, slots, cs), bf16),
            pltpu.VMEM((slots, cs), f32),
            pltpu.VMEM((slots, cs), f32),
            pltpu.VMEM((slots, cs), bf16),
            pltpu.VMEM((slots, cs), bf16),
            pltpu.VMEM((slots, cs), bf16),
            pltpu.VMEM((tp, experts, slots), f32),
            pltpu.VMEM((slots // gate_lanes, experts, gate_lanes), f32),
            dma((10,)), dma((1,)), dma((ep,)), dma((tp, ep)), dma((ep,)), dma((ep,)), dma((ep,)),
            dma((ep,)), dma((ep,)), dma((2, 3)), dma((2, 3)), dma((ep,)), dma((ep,)),
            dma((ep,)), dma((ep,)), dma((tp,)), dma((tp,)), dma((ep,)), dma((ep,)),
        ]
    kept = pl.pallas_call(
        functools.partial(body, ep, tp, cap),
        out_shape=(
            pltpu.VMEM((2, slots, tok_rows), bf16),
            pltpu.VMEM((slots, cs), bf16),
            pltpu.VMEM((ep, per, gate_lanes), f32),
            pltpu.VMEM(w_gate.shape, bf16),
            pltpu.VMEM(w_up.shape, bf16),
            pltpu.VMEM(w_down.shape, bf16),
        ),
        in_specs=[hbm, hbm, small, small, small, hbm, hbm, hbm],
        out_specs=(vmem,) * 6,
        scratch_shapes=scratch,
        compiler_params=pltpu.CompilerParams(
            collective_id=0, has_side_effects=True, vmem_limit_bytes=57 * 1024 * 1024),
    )(tokens, cotangent, gid, wid, gw, w_gate, w_up, w_down)
    dtok, dgate, gwg, gwu, gwd = pl.pallas_call(
        finish,
        out_shape=(
            jax.ShapeDtypeStruct((tok_rows, cs), bf16),
            jax.ShapeDtypeStruct(wid.shape, f32),
            jax.ShapeDtypeStruct(w_gate.shape, bf16),
            jax.ShapeDtypeStruct(w_up.shape, bf16),
            jax.ShapeDtypeStruct(w_down.shape, bf16),
        ),
        in_specs=[vmem] * 8,
        out_specs=(hbm,) * 5,
        scratch_shapes=[
            pltpu.VMEM((tok_rows, cs), bf16),
            pltpu.VMEM(wid.shape, f32),
            dma((2 + 6 * experts,)),
        ],
        compiler_params=pltpu.CompilerParams(vmem_limit_bytes=12 * 1024 * 1024),
    )(*kept, gid, wid)
    return dtok, dgate.T, gwg, gwu, gwd


def solution(mesh):
    in_specs = (
        P("ep", None),
        P("ep", None),
        P("ep", None),
        P("ep", None),
        P("ep", None),
        P("ep", None, "tp"),
        P("ep", None, "tp"),
        P("ep", "tp", None),
    )
    out_specs = (
        P("ep", "tp"),
        P("ep", None),
        P("ep", None, "tp"),
        P("ep", None, "tp"),
        P("ep", "tp", None),
    )
    return jax.shard_map(
        on_device, mesh=mesh, in_specs=in_specs, out_specs=out_specs, check_vma=False
    )
```
